32 devices in a mesh: ep: 8 (over z, x), tp: 4 (over y, core).
Axes of the slice: x: 2, y: 2, z: 4, core: 2. Of those that a mesh axis runs over, the one named last changes fastest.
Arguments:
- mix_query: bfloat16 [2048, 2048], P('ep', 'tp'), may hold values from -6 to 6
- forget_input: bfloat16 [2048, 2048], P('ep', 'tp'), may hold values from -6 to 6
- mix_value: bfloat16 [2048, 2048], P('ep', 'tp'), may hold values from -6 to 6
- out_gate_input: bfloat16 [2048, 2048], P('ep', 'tp'), may hold values from -6 to 6
- decay_shift: float32 [2048, 16], P('ep', 'tp'), may hold values from -1.5 to 0
- forget_floor: float32 [2048], P('tp'), may hold values from 0.9 to 1
- head_gain: float32 [128], replicated, may hold values from 0.1 to 1.9
- w_mix_out: bfloat16 [2048, 2048], P(None, 'tp'), may hold values from -0.125 to 0.125
- moe_input: bfloat16 [2048, 2048], P('ep'), may hold values from -6 to 6
- moe_gain: float32 [2048], replicated, may hold values from 0.1 to 1.9
- routes: int32 [2048, 2], P('ep'), may hold values from 0 to 7, all different within a row; in each aligned block of 256 rows (0 to 255, 256 to 511, ...) at most 80 rows name the same one
- route_weight: float32 [2048, 2], P('ep'), may hold values from 0.1 to 1
- w_exp_gate: bfloat16 [8, 2048, 4096], P('ep', None, 'tp'), may hold values from -0.125 to 0.125
- w_exp_up: bfloat16 [8, 2048, 4096], P('ep', None, 'tp'), may hold values from -0.125 to 0.125
- w_exp_down: bfloat16 [8, 4096, 2048], P('ep', 'tp'), may hold values from -0.125 to 0.125
Outputs:
- mixed: bfloat16 [2048, 2048], P('ep', 'tp')
- moe_out: bfloat16 [2048, 2048], P('ep', 'tp')
The draws below stay inside these ranges and needn't reach their ends.
Inputs may be any that keep to these rules, and one draw needn't show every extreme that they name: `routes`: at most 80 of the rows of one index of ep name one expert, and in every draw some device's rows name one expert exactly 80 times; the experts of a row differ.
All inputs are finite; a program needn't handle non-finite values.
Results may differ from the reference program's by a relative error of at most 0.02.
Values may be sent and summed in bfloat16 or wider, within the bound.
A program may use at most 64 MiB of HBM per device.

```python
import math
import jax
import jax.numpy as jnp
import numpy as np
from jax import lax

D = 2048
HEADS = 16
DK = 128
FE = 4096
TOP_K = 2
BLOCK = 64
TOK_DEV = 256
HW = 2048
TOKENS = 2048
EXPERTS = 8
CAP = 80
N_EP = 8
N_TP = 4


def draw_forget_floor(key, part):
    length = TOK_DEV * N_EP
    subkeys = jax.random.split(key, 3)
    fast_share = 0.5
    fast_heads = jax.random.bernoulli(subkeys[0], fast_share, (HEADS,))
    fast_rate = jnp.exp(jax.random.uniform(subkeys[1], (HEADS, DK), jnp.float32, math.log(0.02), math.log(0.07)))
    slow_rate = jnp.exp(jax.random.uniform(subkeys[2], (HEADS, DK), jnp.float32, math.log(0.3), 0.0)) / length
    keep_rate = jnp.where(fast_heads[:, None], fast_rate, slow_rate)
    return (1.0 - keep_rate).reshape(HEADS * DK).astype(jnp.float32)


def draw_decay_shift(key, part):
    length = TOK_DEV * N_EP
    subkeys = jax.random.split(key, 3)
    factor = jnp.exp(jax.random.uniform(subkeys[0], (N_EP, HEADS), jnp.float32, -math.log(2.0), math.log(2.0)))
    steady = -0.4 * jnp.repeat(factor, TOK_DEV, axis=0) / length
    places = jax.random.randint(subkeys[1], (2, HEADS), 0, length)
    depths = jnp.log(jax.random.uniform(subkeys[2], (2, HEADS), jnp.float32, 0.55, 0.8))
    marked = (jnp.arange(length)[:, None, None] == places[None, :, :]).astype(jnp.float32)
    return (steady + jnp.sum(marked * depths[None, :, :], axis=1)).astype(jnp.float32)


def spiked(result, stream_key, source, target, blocks, factor):
    owner, partner = [(jnp.arange(result.shape[axis_at]) // (result.shape[axis_at] // blocks)).reshape([-1 if axis == axis_at else 1 for axis in range(result.ndim)]) for axis_at in (source, target)]
    chosen = jax.random.permutation(stream_key, blocks)[partner]
    strong = (owner == chosen) | (owner == (partner + blocks // 2) % blocks)
    return jnp.where(strong, factor * result, result)


def block_levels(own_key, extent, pieces, smallest, largest):
    loudness = 1.0
    for dim, shards_of in pieces:
        draws = jax.random.uniform(jax.random.fold_in(jax.random.fold_in(own_key, 6), dim), (shards_of,), jnp.float32, smallest / len(pieces), largest / len(pieces))
        loudness = loudness * jnp.repeat(jnp.exp(draws), extent[dim] // shards_of).reshape((-1,) + (1,) * (len(extent) - 1 - dim))
    return loudness


def assign_block(stream_key, own, number, rows, amount, top, reach, slope):
    sequence = jax.random.permutation(stream_key, amount)
    heavy_load, common = shares(amount, rows * top, reach, slope, True), shares(amount, rows * top, reach, slope, False)
    places = jnp.arange(amount)

    def named(tallies, offset_by):
        used = int((tallies > 0).sum())
        fixed = max(1, used // 4)
        moved = fixed + (places - fixed + offset_by * (used - fixed)) % max(1, amount - fixed)
        return jnp.zeros((amount,), jnp.int32).at[sequence[jnp.where(places < fixed, places, moved)]].set(jnp.asarray(tallies, jnp.int32))

    tallies = jnp.where(number % 4 == 0, named(heavy_load, number // 4), named(common, number - number // 4 - 1))
    mixed = jax.random.permutation(jax.random.fold_in(own, 3), amount)
    donor, taker = mixed[0:amount // 2 * 2:2], mixed[1:amount // 2 * 2:2]
    margin = jnp.minimum(tallies[donor] - 1, reach - tallies[taker]) // 2
    margin = jnp.where((donor == sequence[0]) | (taker == sequence[0]) | (tallies[taker] == 0), 0, jnp.maximum(margin, 0))
    moved = jax.random.randint(jax.random.fold_in(own, 4), (amount // 2,), 0, 1 << 20) % (margin + 1)
    tallies = tallies.at[donor].add(-moved).at[taker].add(moved)
    labels = jnp.searchsorted(jnp.cumsum(tallies), jnp.arange(rows * top), side="right").astype(jnp.int32)
    grid = labels.reshape(top, rows).T
    grid = grid[jax.random.permutation(jax.random.fold_in(own, 1), rows)]
    offset_by = jax.random.randint(jax.random.fold_in(own, 2), (rows, 1), 0, top)
    return jnp.take_along_axis(grid, (jnp.arange(top)[None, :] + offset_by) % top, axis=1)


def shares(number_of, total, bound, skew, full):
    portions = [(1 << 20) // math.isqrt(rank ** skew) + 1 for rank in range(1, number_of + 1)]
    largest = bound if full else min(bound, max(-(-total // number_of), total * portions[0] // sum(portions)))
    least = 1 if total - largest >= number_of - 1 else 0
    given, rest = [largest] + [least] * (number_of - 1), total - largest - least * (number_of - 1)
    while rest > 0:
        movable = [i for i in range(1, number_of) if given[i] < largest] or [i for i in range(1, number_of) if given[i] < bound]
        mass, remaining = sum([portions[i] for i in movable]), rest
        for i in movable:
            addition = min(bound - given[i], max(1, remaining * portions[i] // mass), rest)
            given[i] = given[i] + addition
            rest = rest - addition
    return np.array(given)


def centred(stream_key, extent, scale, bound, pieces=(), kind=jnp.bfloat16):
    drawn = scale * jax.random.normal(stream_key, extent, jnp.float32)
    if pieces:
        drawn = drawn * block_levels(stream_key, extent, pieces, -0.22, 0.18)
    return jnp.clip(drawn, -bound, bound).astype(kind)


def bell_draw_with(key, shape, scale, reach, cuts, heavy, held_as=jnp.bfloat16):
    values = scale * jax.random.normal(key, shape, jnp.float32)
    if cuts:
        values = values * block_levels(key, shape, cuts, -0.22, 0.18)
    return jnp.clip(spiked(values, jax.random.fold_in(key, 3), *heavy), -reach, reach).astype(held_as)


def setup_inputs(seed: int = 0) -> dict:
    key_of = jax.random.split(jax.random.key(seed), 16)
    mix_query = centred(key_of[0], (TOKENS, HW), 1.0, 6.0, ((0, 8), (1, 4)))
    forget_input = centred(key_of[1], (TOKENS, HW), 1.0, 6.0, ((0, 8), (1, 4)))
    mix_value = centred(key_of[2], (TOKENS, HW), 1.0, 6.0, ((0, 8), (1, 4)))
    out_gate_input = centred(key_of[3], (TOKENS, HW), 1.0, 6.0, ((0, 8), (1, 4)))
    decay_shift = draw_decay_shift(jax.random.fold_in(key_of[15], 71), 0)
    forget_floor = draw_forget_floor(jax.random.fold_in(key_of[15], 71), 0)
    head_gain = jnp.clip(1.0 + 0.18 * jax.random.normal(key_of[6], (DK,), jnp.float32), 0.1, 1.9)
    w_mix_out = centred(key_of[7], (HW, D), HW ** -0.5, 0.125, ((1, 4),))
    moe_input = centred(key_of[8], (TOKENS, D), 1.0, 6.0, ((0, 8),))
    moe_gain = jnp.clip(1.0 + 0.18 * jax.random.normal(key_of[9], (D,), jnp.float32), 0.1, 1.9)
    routes_keys = jax.random.split(jax.random.fold_in(key_of[10], 1), TOKENS // TOK_DEV)
    routes_turns = jax.random.permutation(jax.random.fold_in(key_of[10], 3), TOKENS // TOK_DEV)
    routes = jax.vmap(lambda own, number: assign_block(jax.random.fold_in(key_of[10], 2), own, number, TOK_DEV, EXPERTS, TOP_K, CAP, 1))(routes_keys, routes_turns).reshape((TOKENS, TOP_K))
    route_weight = jnp.clip(0.1 + 0.9 * jax.random.uniform(key_of[11], (TOKENS, TOP_K), jnp.float32) ** block_levels(key_of[11], (TOKENS, TOP_K), ((0, 8),), -0.2, 0.2), 0.1, 1.0)
    w_exp_gate = centred(key_of[12], (EXPERTS, D, FE), D ** -0.5, 0.125, ((0, 8), (2, 4)))
    w_exp_up = centred(key_of[13], (EXPERTS, D, FE), D ** -0.5, 0.125, ((0, 8), (2, 4)))
    w_exp_down = bell_draw_with(key_of[14], (EXPERTS, FE, D), FE ** -0.5, 0.125, ((0, 8), (1, 4)), (1, 2, 4, 2.0))
    return {"mix_query": mix_query, "forget_input": forget_input, "mix_value": mix_value, "out_gate_input": out_gate_input, "decay_shift": decay_shift, "forget_floor": forget_floor, "head_gain": head_gain, "w_mix_out": w_mix_out, "moe_input": moe_input, "moe_gain": moe_gain, "routes": routes, "route_weight": route_weight, "w_exp_gate": w_exp_gate, "w_exp_up": w_exp_up, "w_exp_down": w_exp_down}


eps = 1e-06
highest_precision = lax.Precision.HIGHEST

def recurrence(query, input_gate, values, log_decay):
    length = query.shape[0]
    blocks = length // BLOCK

    def to_blocks(array):
        return array.reshape(blocks, BLOCK, HEADS, DK).transpose(0, 2, 1, 3)
    causal = jnp.tril(jnp.ones((BLOCK, BLOCK), bool))[:, :, None]

    def advance(recurrent_state, inputs):
        query_block, key_block, value_block, g_block = inputs
        running_decay = jnp.cumsum(g_block, axis=1)
        spread = running_decay[:, :, None, :] - running_decay[:, None, :, :]
        weights = jnp.where(causal, jnp.exp(jnp.minimum(spread, 0.0)), 0.0)
        scores = jnp.einsum('htk,htsk,hsk->hts', query_block, weights, key_block, precision=highest_precision)
        block_result = jnp.einsum('hts,hsv->htv', scores, value_block, precision=highest_precision)
        block_result = block_result + jnp.einsum('rsd,rda->rsa', query_block * jnp.exp(running_decay), recurrent_state, precision=highest_precision)
        closing_total = running_decay[:, -1:, :]
        carried_over_state = jnp.einsum('gbx,gbi->gxi', key_block * jnp.exp(closing_total - running_decay), value_block, precision=highest_precision)
        recurrent_state = jnp.exp(closing_total[:, 0, :])[:, :, None] * recurrent_state + carried_over_state
        return (recurrent_state, block_result)
    initial = jnp.zeros((HEADS, DK, DK), jnp.float32)
    _, block_result = lax.scan(advance, initial, (to_blocks(query), to_blocks(input_gate), to_blocks(values), to_blocks(log_decay)))
    return block_result.transpose(0, 2, 1, 3).reshape(length, HEADS, DK)

def token_mixer(mix_query, forget_input, mix_value, out_gate_input, decay_shift, forget_floor, head_gain, w_mix_out):
    length = mix_query.shape[0]
    gate_input = forget_input.astype(jnp.float32)
    forget = forget_floor + (1.0 - forget_floor) * jax.nn.sigmoid(gate_input)
    input_gate = (1.0 - forget_floor) * jax.nn.sigmoid(-gate_input)
    log_decay = jnp.log(forget) + jnp.repeat(decay_shift, DK, axis=1)
    block_result = recurrence(mix_query.astype(jnp.float32), input_gate, mix_value.astype(jnp.float32), log_decay)
    inverse = lax.rsqrt(lax.optimization_barrier(jnp.mean(block_result * block_result, axis=2, keepdims=True)) + eps)
    gated = jax.nn.silu(out_gate_input.astype(jnp.float32)).reshape(length, HEADS, DK)
    head_out = (block_result * inverse * head_gain * gated).reshape(length, HEADS * DK).astype(jnp.bfloat16)
    return jnp.dot(head_out, w_mix_out, preferred_element_type=jnp.float32).astype(jnp.bfloat16)

def experts_layer(moe_input, moe_gain, routes, route_weight, w_exp_gate, w_exp_up, w_exp_down):
    token_rows = moe_input.astype(jnp.float32)
    inverse = lax.rsqrt(lax.optimization_barrier(jnp.mean(token_rows * token_rows, axis=1, keepdims=True)) + eps)
    normed = (token_rows * inverse * moe_gain).astype(jnp.bfloat16)
    flat_ids = routes.reshape(-1)
    pair_count = flat_ids.shape[0]
    slot_count = CAP * N_EP
    group_size = FE // N_TP

    def one_expert(expert):
        matches = flat_ids == expert
        chosen = jnp.nonzero(matches, size=slot_count, fill_value=0)[0].astype(jnp.int32)
        how_many = jnp.sum(matches.astype(jnp.int32))
        usable = jnp.arange(slot_count, dtype=jnp.int32) < how_many
        picked = normed[chosen // TOP_K]
        gate_sum = jnp.dot(picked, w_exp_gate[expert], preferred_element_type=jnp.float32)
        up_sum = jnp.dot(picked, w_exp_up[expert], preferred_element_type=jnp.float32)
        hidden = (jax.nn.silu(gate_sum) * up_sum).astype(jnp.bfloat16)
        grouped = hidden.reshape(slot_count, N_TP, group_size).astype(jnp.float32)
        down_groups = w_exp_down[expert].reshape(N_TP, group_size, D).astype(jnp.float32)
        partial_value = jnp.einsum('sgf,gfd->sgd', grouped, down_groups).astype(jnp.bfloat16)
        summed = lax.optimization_barrier(jnp.sum(partial_value.astype(jnp.float32), axis=1)).astype(jnp.bfloat16)
        return (chosen, jnp.where(usable[:, None], summed, jnp.zeros_like(summed)))
    chosen_all, outputs = lax.map(one_expert, jnp.arange(EXPERTS, dtype=jnp.int32))
    pair_out = jnp.zeros((pair_count, D), jnp.float32).at[chosen_all.reshape(-1)].add(outputs.reshape(-1, D).astype(jnp.float32))
    combined = lax.optimization_barrier(jnp.sum(pair_out.reshape(-1, TOP_K, D) * route_weight[:, :, None], axis=1))
    return combined.astype(jnp.bfloat16)

def reference(mix_query, forget_input, mix_value, out_gate_input, decay_shift, forget_floor, head_gain, w_mix_out, moe_input, moe_gain, routes, route_weight, w_exp_gate, w_exp_up, w_exp_down):
    mixed = token_mixer(mix_query, forget_input, mix_value, out_gate_input, decay_shift, forget_floor, head_gain, w_mix_out)
    moe_out = experts_layer(moe_input, moe_gain, routes, route_weight, w_exp_gate, w_exp_up, w_exp_down)
    return (mixed, moe_out)
```

```python
import functools

import jax
import jax.numpy as jnp
from jax import lax
from jax.experimental import pallas as pl
from jax.experimental.pallas import tpu as pltpu
from jax.sharding import PartitionSpec as P

TOP_K = 2
EPS = 1e-06
MESH = pl.DeviceIdType.MESH
BF = jnp.bfloat16
F32 = jnp.float32
HIGH = lax.Precision.HIGHEST
NS = jax.named_scope


def mm(a, b, dims=((1,), (0,)), precision=None):
    return lax.dot_general(
        a, b, (dims, ((), ())), preferred_element_type=F32, precision=precision
    )


def kernel(
    cfg,
    q_hbm,
    fi_hbm,
    v_hbm,
    og_hbm,
    ds_hbm,
    ff_hbm,
    hg_hbm,
    x_hbm,
    mg_hbm,
    rt_hbm,
    rw_hbm,
    wm_hbm,
    wg_hbm,
    wu_hbm,
    wd_hbm,
    mixed_hbm,
    moe_hbm,
    q_ref,
    fi_ref,
    v_ref,
    og_ref,
    ds_ref,
    ff_ref,
    hg_ref,
    x_ref,
    mg_ref,
    rt_ref,
    rw_ref,
    mixed_ref,
    moe_ref,
    wm,
    wg,
    wu,
    wd,
    dispn,
    dispf,
    xs,
    hid,
    snd_p,
    rs_p,
    own,
    snd_y,
    rs_y,
    fin,
    ret,
    wpn,
    wpf,
    kx_s,
    kx_r,
    kc_s,
    kc_r,
    pair,
    carry,
    intra,
    qdec,
    ho,
    in_sem,
    out_sem,
    w_sem,
    a_ss,
    a_rs,
    gy_ss,
    gy_rs,
    gp_ss,
    gp_rs,
    rp_ss,
    rp_rs,
    ry_ss,
    ry_rs,
    b_ss,
    b_rs,
    kx_ss,
    kx_rs,
    kc_ss,
    kc_rs,
    hy_ss,
    hy_rs,
    hp_ss,
    hp_rs,
):
    ep, tp, cap, near = cfg
    far = ep - near
    ny = tp // 2
    me = lax.axis_index("ep")
    t = lax.axis_index("tp")
    y = t // 2
    c = t % 2
    mate = y * 2 + (1 - c)
    rows, dim = x_ref.shape
    width = dim // tp
    slots = ep * cap
    hidden_units = wg.shape[1]
    heads = ds_ref.shape[0]
    hs = hg_ref.shape[1]
    hw = q_ref.shape[1]
    hpn = ho.shape[2]
    cw = hw // hpn
    bits = ep.bit_length() - 1
    me_bits = [lax.rem(lax.div(me, 2**k), 2) for k in range(bits)]
    zi = lax.div(me, 2)
    nz = ep // 2
    xb = me_bits[0]

    def ring(a, n):
        return lax.rem(a + n, n)

    def up_y(dy):
        return ring(y + dy, ny)

    def dn_y(dy):
        return ring(y - dy, ny)

    def peer(mask):
        out = 0
        for k in range(bits):
            out = out + (1 - me_bits[k] if (mask >> k) & 1 else me_bits[k]) * 2**k
        return out

    def peer_dyn(mask):
        out = 0
        for k in range(bits):
            m = lax.rem(lax.div(mask, 2**k), 2)
            out = out + lax.rem(me_bits[k] + m, 2) * 2**k
        return out

    def rc(src, dst, ss, rs, e, j):
        return pltpu.make_async_remote_copy(
            src_ref=src, dst_ref=dst, send_sem=ss, recv_sem=rs, device_id=(e, j), device_id_type=MESH
        )

    loads = [
        pltpu.make_async_copy(wg_hbm.at[0], wg, w_sem.at[0]),
        pltpu.make_async_copy(wu_hbm.at[0], wu, w_sem.at[1]),
        pltpu.make_async_copy(wd_hbm.at[0], wd, w_sem.at[2]),
        pltpu.make_async_copy(wm_hbm, wm, w_sem.at[3]),
    ]
    small = {}
    pairs = (
        ("rt", rt_hbm, rt_ref),
        ("x", x_hbm, x_ref),
        ("mg", mg_hbm, mg_ref),
        ("fi", fi_hbm, fi_ref),
        ("ff", ff_hbm, ff_ref),
        ("ds", ds_hbm, ds_ref),
        ("v", v_hbm, v_ref),
        ("q", q_hbm, q_ref),
        ("rw", rw_hbm, rw_ref),
        ("og", og_hbm, og_ref),
        ("hg", hg_hbm, hg_ref),
    )
    for i, (name, src, dst) in enumerate(pairs):
        small[name] = pltpu.make_async_copy(src, dst, in_sem.at[i])
    for name in ("rt", "x", "mg"):
        small[name].start()
    barrier = pltpu.get_barrier_semaphore()
    for d in range(1, ep):
        pl.semaphore_signal(barrier, inc=1, device_id=(ring(me + d, ep), t), device_id_type=MESH)
    for dy in range(1, ny):
        pl.semaphore_signal(barrier, inc=1, device_id=(me, up_y(dy) * 2 + c), device_id_type=MESH)
    pl.semaphore_signal(barrier, inc=1, device_id=(me, mate), device_id_type=MESH)

    gn, gf = near // 2, far // 2
    inner = lax.rem(me_bits[1] + me_bits[2], 2) if bits > 2 else 0
    groups = [
        (0, gn, 0, True),
        (near + gf * (1 - inner), gf, gn * cap, False),
        (gn, gn, (gn + gf) * cap, True),
        (near + gf * inner, gf, (2 * gn + gf) * cap, False),
    ]

    def a2a(p):
        if p < near:
            return rc(dispn.at[:, p], xs.at[:, c, p], a_ss.at[p], a_rs.at[p], peer(p), t)
        return rc(dispf.at[p - near], xs.at[y, c, p], a_ss.at[p], a_rs.at[p], peer(p), t)

    def a2a_in(p, is_near):
        r = xs.at[:, c, p] if is_near else xs.at[y, c, p]
        return rc(r, r, a_ss.at[p], a_rs.at[p], me, mate)

    def near_p(p):
        r = xs.at[:, c, p]
        return rc(r, r, gp_ss.at[0, p], gp_rs.at[0, p], me, mate)

    def near_p_in(p):
        r = xs.at[:, 1 - c, p]
        return rc(r, r, gp_ss.at[0, p], gp_rs.at[0, p], me, mate)

    def gat_y(p, dy):
        r = xs.at[y, c, p]
        return rc(r, r, gy_ss.at[dy, p], gy_rs.at[dy, p], me, up_y(dy) * 2 + c)

    def gat_y_in(p, dy):
        r = xs.at[dn_y(dy), c, p]
        return rc(r, r, gy_ss.at[dy, p], gy_rs.at[dy, p], me, mate)

    def gat_p(p, dy):
        r = xs.at[dn_y(dy), c, p]
        return rc(r, r, gp_ss.at[dy, p], gp_rs.at[dy, p], me, mate)

    def gat_p_in(p, dy):
        r = xs.at[dn_y(dy), 1 - c, p]
        return rc(r, r, gp_ss.at[dy, p], gp_rs.at[dy, p], me, mate)

    def take_near(p):
        with NS(f"take_near{p}"):
            if p:
                a2a_in(p, True).wait_recv()
            near_p(p).start()

    def take_far(g, i):
        with NS(f"take_far{g}"):
            p = groups[g][0] + i
            a2a_in(p, False).wait_recv()
            for dy in range(1, ny):
                gat_y(p, dy).start()
            gat_p(p, 0).start()

    def relay_far(g, i):
        with NS(f"relay_far{g}"):
            p = groups[g][0] + i
            for dy in range(1, ny):
                gat_y_in(p, dy).wait_recv()
                gat_p(p, dy).start()

    def arrived(g):
        with NS(f"arrived{g}"):
            base, n, _, is_near = groups[g]
            for i in range(n):
                if is_near:
                    near_p_in(base + i).wait_recv()
                else:
                    for dy in range(ny):
                        gat_p_in(base + i, dy).wait_recv()

    with NS("rt_wait"):
        small["rt"].wait()
    with NS("route"):
        i_r = lax.broadcasted_iota(jnp.int32, (rows, rows), 0)
        i_c = lax.broadcasted_iota(jnp.int32, (rows, rows), 1)
        hr = max(8, ep)
        p_row = lax.broadcasted_iota(jnp.int32, (hr, rows), 0)
        pos, hot = [], []
        for k in range(TOP_K):
            r = jnp.bitwise_xor(rt_ref[k : k + 1, :], me)
            pos.append(r)
            hot.append((p_row == r).astype(F32))
        before = mm(sum(hot).astype(BF), (i_r < i_c).astype(F32).astype(BF))
        slot = []
        for k in range(TOP_K):
            rank = jnp.sum(before * hot[k], axis=0, keepdims=True).astype(jnp.int32)
            slot.append(pos[k] * cap + rank)
        s_row = lax.broadcasted_iota(jnp.int32, (slots, rows), 0)
        hits = [s_row == slot[k] for k in range(TOP_K)]
        pick = jnp.where(hits[0], 1.0, jnp.where(hits[1], 1.0, 0.0)).astype(BF)
    with NS("x_wait"):
        small["x"].wait()
        small["mg"].wait()
        for name in ("fi", "ff", "ds", "v", "q", "rw", "og", "hg"):
            small[name].start()
    with NS("norm"):
        xf = x_ref[...].astype(F32)
        inv = lax.rsqrt(jnp.mean(xf * xf, axis=1, keepdims=True) + EPS)

        def normed(yy):
            cols = pl.ds(pl.multiple_of((yy * 2 + c) * width, width), width)
            return (x_ref[:, cols].astype(F32) * inv * mg_ref[:, cols]).astype(BF)

    nr = near * cap
    with NS("disp_near"):
        for yy in range(ny):
            out = mm(pick[0:nr], normed(yy)).astype(BF).reshape(near, cap, width)
            dispn[yy] = out
            xs[yy, c, 0] = out[0]
    with NS("bar"):
        pl.semaphore_wait(barrier, ep - 1 + ny)
    for p in range(1, gn):
        a2a(p).start()
    with NS("disp_far"):
        dispf[...] = mm(pick[nr:], normed(y)).astype(BF).reshape(far, cap, width)
    for p in list(range(near, ep)) + list(range(gn, near)):
        a2a(p).start()
    take_near(0)

    causal = i_r >= i_c
    tri = causal.astype(F32)

    def mix_all_decay():
        fl = ff_ref[...]
        fx = fi_ref[...].astype(F32)
        forget = fl + (1.0 - fl) * jax.nn.sigmoid(fx)
        return mm(tri, jnp.log(forget), precision=HIGH)

    def state_x(h):
        return rc(kx_s.at[h], kx_r.at[h], kx_ss.at[h], kx_rs.at[h], peer(1), t)

    def mix_head(h, run, s_col, s_row):
        hc = slice(h * hs, (h + 1) * hs)
        lr = run[:, hc]
        sc = s_col[:, h : h + 1]
        sr = s_row[h : h + 1, :]
        key = (1.0 - ff_ref[:, hc]) * jax.nn.sigmoid(-fi_ref[:, hc].astype(F32))
        v = v_ref[:, hc]
        l_end = lr[rows - 1 : rows, :]
        s_end = sc[rows - 1 : rows, :]
        kd = (key * jnp.exp(l_end - lr + (s_end - sc))).astype(BF)
        kx_s[h, 0:hs, :] = mm(v, kd, ((0,), (0,))).astype(BF)
        kx_s[h, hs : hs + 16, :] = jnp.broadcast_to(jnp.exp(l_end + s_end), (16, hs)).astype(BF)
        state_x(h).start()
        q = q_ref[:, hc].astype(F32) * jnp.exp(lr)
        scores = mm(q.astype(BF), (key * jnp.exp(-lr)).astype(BF), ((1,), (1,)))
        scores = jnp.where(causal, scores * jnp.exp(jnp.minimum(sc - sr, 0.0)), 0.0)
        intra[:, hc] = mm(scores.astype(BF), v)
        qdec[:, hc] = (q * jnp.exp(sc)).astype(BF)

    with NS("mix_wait"):
        for name in ("fi", "ff", "ds", "v", "q", "rw", "og", "hg"):
            small[name].wait()
        for load in loads:
            load.start()
    with NS("decay"):
        run = mix_all_decay()
        s_col = mm(tri, ds_ref[...], ((1,), (1,)), HIGH)
        s_rows = mm(ds_ref[...], tri, ((1,), (1,)), HIGH)
    for h in range(heads):
        with NS(f"head{h}"):
            mix_head(h, run, s_col, s_rows)
    with NS("weights"):
        wp = jnp.where(hits[0], rw_ref[0:1, :], jnp.where(hits[1], rw_ref[1:2, :], 0.0))
        wpn[...] = wp[0:nr].T.astype(BF)
        wpf[...] = wp[nr:].T.astype(BF)

    def chain_copy(h):
        return rc(kc_s.at[h], kc_r.at[h], kc_ss.at[h], kc_rs.at[h], ring(me + 2, ep), t)

    def pair_states():
        for h in range(heads):
            with NS("state_wait"):
                state_x(h).wait_recv()
            mine = kx_s[h].astype(F32)
            other = kx_r[h].astype(F32)
            one = jnp.where(xb == 0, mine, other)
            two = jnp.where(xb == 0, other, mine)
            a_two = two[hs : hs + 1]
            both = a_two * one[0:hs] + two[0:hs]
            pair[h, 0:hs, :] = both
            pair[h, hs : hs + 8, :] = a_two * one[hs : hs + 8]

            @pl.when(zi == 0)
            def _():
                carry[h] = jnp.where(xb == 0, 0.0, other[0:hs]).astype(BF)
                kc_s[h] = both.astype(BF)
                chain_copy(h).start()

    def chain(s):
        @pl.when(zi == s)
        def _():
            for h in range(heads):
                chain_copy(h).wait_recv()
                p = kc_r[h].astype(F32)
                if s + 1 < nz:
                    kc_s[h] = (pair[h, hs : hs + 1, :] * p + pair[h, 0:hs, :]).astype(BF)
                    chain_copy(h).start()
                other = kx_r[h].astype(F32)
                carry[h] = jnp.where(xb == 0, p, other[hs : hs + 1] * p + other[0:hs]).astype(BF)

    def ho_y(p, dy):
        r = ho.at[y, c, p]
        return rc(r, r, hy_ss.at[p, dy], hy_rs.at[p, dy], me, up_y(dy) * 2 + c)

    def ho_y_in(p, dy):
        r = ho.at[dn_y(dy), c, p]
        return rc(r, r, hy_ss.at[p, dy], hy_rs.at[p, dy], me, mate)

    def ho_p(p, dy):
        r = ho.at[dn_y(dy), c, p]
        return rc(r, r, hp_ss.at[p, dy], hp_rs.at[p, dy], me, mate)

    def ho_p_in(p, dy):
        r = ho.at[dn_y(dy), 1 - c, p]
        return rc(r, r, hp_ss.at[p, dy], hp_rs.at[p, dy], me, mate)

    def mix_close():
        for p in range(hpn):
            with NS("close"):
                for i in range(cw // hs):
                    h = p * (cw // hs) + i
                    hc = slice(h * hs, (h + 1) * hs)
                    o = intra[:, hc] + mm(qdec[:, hc], carry[h], ((1,), (1,)))
                    iv = lax.rsqrt(jnp.mean(o * o, axis=1, keepdims=True) + EPS)
                    g = og_ref[:, hc].astype(F32)
                    ho[y, c, p, :, i * hs : (i + 1) * hs] = (
                        o * iv * hg_ref[...] * (g * jax.nn.sigmoid(g))
                    ).astype(BF)
                for dy in range(1, ny):
                    ho_y(p, dy).start()
                ho_p(p, 0).start()

    def ho_relay():
        with NS("ho_relay"):
            for p in range(hpn):
                for dy in range(1, ny):
                    ho_y_in(p, dy).wait_recv()
                    ho_p(p, dy).start()

    def project():
        with NS("ho_wait"):
            for p in range(hpn):
                for dy in range(ny):
                    ho_p_in(p, dy).wait_recv()
        with NS("proj"):
            acc = jnp.zeros(mixed_ref.shape, F32)
            for j in range(tp):
                for p in range(hpn):
                    k0 = j * hw + p * cw
                    acc += mm(ho[j // 2, j % 2, p], wm[k0 : k0 + cw, :])
            mixed_ref[...] = acc.astype(BF)
            pltpu.make_async_copy(mixed_ref, mixed_hbm, out_sem.at[0]).start()

    ft = min(256, hidden_units)

    tiles = hidden_units // ft

    def first(g, between=None):
        if between is None:
            first_part(g, 0, tiles)
        else:
            first_part(g, 0, tiles // 2)
            between()
            first_part(g, tiles // 2, tiles)

    def first_part(g, lo, hi):
        with NS(f"first{g}"):
            base, n, _, is_near = groups[g]
            gr = n * cap

            def tile(k, _):
                fc = pl.ds(pl.multiple_of(k * ft, ft), ft)
                gate = jnp.zeros((gr, ft), F32)
                up = jnp.zeros((gr, ft), F32)
                for j in range(tp):
                    a = xs[j // 2, j % 2, pl.ds(base, n)].reshape(gr, width)
                    gate += mm(a, wg[j * width : (j + 1) * width, fc])
                    up += mm(a, wu[j * width : (j + 1) * width, fc])
                hid[0:gr, fc] = (gate * jax.nn.sigmoid(gate) * up).astype(BF)
                return 0

            lax.fori_loop(lo, hi, tile, 0)

    def red_p(g, dy):
        _, n, r0, _ = groups[g]
        rs = pl.ds(r0, n * cap)
        return rc(snd_p.at[dy, rs], rs_p.at[dy, rs], rp_ss.at[g, dy], rp_rs.at[g, dy], me, mate)

    def red_y(g, i, dy):
        r0 = groups[g][2] + i * cap
        b = r0 // cap
        rs = pl.ds(r0, cap)
        return rc(
            snd_y.at[dy, rs], rs_y.at[dy, rs], ry_ss.at[b, dy], ry_rs.at[b, dy], me, up_y(dy) * 2 + c
        )

    order = list(range(1, ny)) + [0]

    def second(g):
        _, n, r0, _ = groups[g]
        gr = n * cap

        def down(dy, core):
            col = up_y(dy) * 2 + core
            return mm(hid[0:gr], wd[:, pl.ds(pl.multiple_of(col * width, width), width)])

        with NS(f"second{g}"):
            for dy in order:
                snd_p[dy, r0 : r0 + gr] = down(dy, 1 - c).astype(BF)
                red_p(g, dy).start()
            for dy in order:
                own[dy, r0 : r0 + gr] = down(dy, c)

    def reduce_p(g):
        _, n, r0, _ = groups[g]
        with NS(f"reduce_p{g}"):
            for dy in order:
                red_p(g, dy).wait_recv()
                for i in range(n):
                    rr = slice(r0 + i * cap, r0 + (i + 1) * cap)
                    total = own[dy, rr] + rs_p[dy, rr].astype(F32)
                    if dy:
                        snd_y[dy, rr] = total.astype(BF)
                        red_y(g, i, dy).start()
                    else:
                        own[0, rr] = total

    def back(g, i):
        base, _, r0, is_near = groups[g]
        b = r0 // cap + i
        p = base + i
        dest = peer(p) if is_near else peer_dyn(p)
        return rc(fin.at[b], ret.at[p], b_ss.at[b], b_rs.at[p], dest, t)

    def give_back(g):
        _, n, r0, _ = groups[g]
        with NS(f"give_back{g}"):
            for i in range(n):
                rr = slice(r0 + i * cap, r0 + (i + 1) * cap)
                total = own[0, rr]
                for dy in range(1, ny):
                    red_y(g, i, dy).wait_recv()
                    total += rs_y[dy, rr].astype(F32)
                if g == 0 and i == 0:
                    ret[0] = total.astype(BF)
                else:
                    fin[r0 // cap + i] = total.astype(BF)
                    back(g, i).start()

    def back_in(p):
        return rc(fin.at[p], ret.at[p], b_ss.at[p], b_rs.at[p], me, mate)

    def far_taken(g):
        for i in range(gf):
            take_far(g, i)

    def far_relayed(g):
        for i in range(gf):
            relay_far(g, i)

    def chain_at(lo, hi):
        with NS(f"chain{lo}"):
            for s in range(lo, min(hi, nz)):
                chain(s)

    for p in range(1, gn):
        take_near(p)
    with NS("loads"):
        for load in loads[:3]:
            load.wait()
    arrived(0)
    first(0, lambda: take_far(1, 0))
    for i in range(1, gf):
        take_far(1, i)
    second(0)
    with NS("pair_states"):
        pair_states()
    far_relayed(1)
    reduce_p(0)
    arrived(1)
    first(1)
    for p in range(gn, near):
        take_near(p)
    far_taken(3)
    second(1)
    chain_at(1, 2)
    give_back(0)
    reduce_p(1)
    arrived(2)
    first(2)
    far_relayed(3)
    second(2)
    chain_at(2, 3)
    reduce_p(2)
    arrived(3)
    first(3)
    give_back(1)
    second(3)
    chain_at(3, nz)
    reduce_p(3)
    mix_close()
    give_back(2)
    give_back(3)
    ho_relay()
    loads[3].wait()
    project()
    with NS("near_back"):
        for p in range(1, near):
            back_in(p).wait_recv()
    with NS("comb_near"):
        res = mm(wpn[...], ret[0:near].reshape(nr, width))
    with NS("far_back"):
        for p in range(near, ep):
            back_in(p).wait_recv()
    with NS("comb_far"):
        res += mm(wpf[...], ret[near:].reshape(slots - nr, width))
        moe_ref[...] = res.astype(BF)
        pltpu.make_async_copy(moe_ref, moe_hbm, out_sem.at[1]).start()

    with NS("drain"):
        for p in range(1, ep):
            a2a(p).wait_send()
        for g, (base, n, r0, is_near) in enumerate(groups):
            for i in range(n):
                if g or i:
                    back(g, i).wait_send()
                for dy in range(1, ny):
                    red_y(g, i, dy).wait_send()
                if is_near:
                    near_p(base + i).wait_send()
                else:
                    for dy in range(ny):
                        gat_p(base + i, dy).wait_send()
                        if dy:
                            gat_y(base + i, dy).wait_send()
            for dy in range(ny):
                red_p(g, dy).wait_send()
        for h in range(heads):
            state_x(h).wait_send()
            pl.when(zi + 1 < nz)(lambda h=h: chain_copy(h).wait_send())
        for p in range(hpn):
            for dy in range(ny):
                ho_p(p, dy).wait_send()
                if dy:
                    ho_y(p, dy).wait_send()
        pltpu.make_async_copy(mixed_ref, mixed_hbm, out_sem.at[0]).wait()
        pltpu.make_async_copy(moe_ref, moe_hbm, out_sem.at[1]).wait()


def emit(a_ref, b_ref, a_out, b_out, held, sem):
    copies = [
        (
            pltpu.make_async_copy(src, held.at[i], sem.at[i, 0]),
            pltpu.make_async_copy(held.at[i], dst, sem.at[i, 1]),
        )
        for i, (src, dst) in enumerate(((a_ref, a_out), (b_ref, b_out)))
    ]
    for take, _ in copies:
        take.start()
    for take, give in copies:
        take.wait()
        give.start()
    for _, give in copies:
        give.wait()


def body(ep, tp, *args):
    (q, fi, v, og, ds, ff, hg, wm, x, mg, rt, rw, wg, wu, wd) = args
    rows, dim = x.shape
    capacity = 5 * rows * TOP_K // (4 * ep)
    cap = -(-capacity // 16) * 16
    near = min(4, ep // 2)
    ny = tp // 2
    width = dim // tp
    heads = ds.shape[1]
    hs = hg.shape[0]
    hw = q.shape[1]
    hpn = max(1, heads // 2)
    fu = wg.shape[2]
    slots = ep * cap
    gmax = max(near // 2, (ep - near) // 2) * cap
    vm = pltpu.VMEM
    dma = pltpu.SemaphoreType.DMA
    operands = (q, fi, v, og, ds.T, ff[None, :], hg[None, :], x, mg[None, :], rt.T, rw.T)
    scratch = [vm(a.shape, a.dtype) for a in operands] + [
        vm((rows, width), BF),
        vm((rows, width), BF),
        vm(wm.shape, BF),
        vm(wg.shape[1:], BF),
        vm(wu.shape[1:], BF),
        vm(wd.shape[1:], BF),
        vm((ny, near, cap, width), BF),
        vm((ep - near, cap, width), BF),
        vm((ny, 2, ep, cap, width), BF),
        vm((gmax, fu), BF),
        vm((ny, slots, width), BF),
        vm((ny, slots, width), BF),
        vm((ny, slots, width), F32),
        vm((ny, slots, width), BF),
        vm((ny, slots, width), BF),
        vm((ep, cap, width), BF),
        vm((ep, cap, width), BF),
        vm((rows, near * cap), BF),
        vm((rows, slots - near * cap), BF),
        vm((heads, hs + 16, hs), BF),
        vm((heads, hs + 16, hs), BF),
        vm((heads, hs, hs), BF),
        vm((heads, hs, hs), BF),
        vm((heads, hs + 8, hs), F32),
        vm((heads, hs, hs), BF),
        vm((rows, hw), F32),
        vm((rows, hw), BF),
        vm((ny, 2, hpn, rows, hw // hpn), BF),
        dma((len(operands),)),
        dma((2,)),
        dma((4,)),
        dma((ep,)),
        dma((ep,)),
        dma((ny, ep)),
        dma((ny, ep)),
        dma((ny, ep)),
        dma((ny, ep)),
        dma((4, ny)),
        dma((4, ny)),
        dma((ep, ny)),
        dma((ep, ny)),
        dma((ep,)),
        dma((ep,)),
        dma((heads,)),
        dma((heads,)),
        dma((heads,)),
        dma((heads,)),
        dma((hpn, ny)),
        dma((hpn, ny)),
        dma((hpn, ny)),
        dma((hpn, ny)),
    ]
    out = jax.ShapeDtypeStruct((rows, width), BF)
    in_any = pl.BlockSpec(memory_space=pl.ANY)
    made = pl.pallas_call(
        functools.partial(kernel, (ep, tp, cap, near)),
        out_shape=(out, out),
        in_specs=[in_any] * 15,
        out_specs=(in_any, in_any),
        scratch_shapes=scratch,
        compiler_params=pltpu.CompilerParams(
            collective_id=0, has_side_effects=True, vmem_limit_bytes=60 * 1024 * 1024
        ),
    )(*operands, wm, wg, wu, wd)
    return pl.pallas_call(
        emit,
        out_shape=(out, out),
        in_specs=[in_any] * 2,
        out_specs=(in_any, in_any),
        scratch_shapes=[vm((2, rows, width), BF), dma((2, 2))],
        name="emit",
    )(*made)


def solution(mesh):
    placed = (
        P("ep", "tp"),
        P("ep", "tp"),
        P("ep", "tp"),
        P("ep", "tp"),
        P("ep", "tp"),
        P("tp"),
        P(),
        P(None, "tp"),
        P("ep", None),
        P(),
        P("ep", None),
        P("ep", None),
        P("ep", None, "tp"),
        P("ep", None, "tp"),
        P("ep", "tp", None),
    )
    return jax.shard_map(
        functools.partial(body, mesh.shape["ep"], mesh.shape["tp"]),
        mesh=mesh,
        in_specs=placed,
        out_specs=(P("ep", "tp"), P("ep", "tp")),
        check_vma=False,
    )
```

```python
import functools

import jax
import jax.numpy as jnp
from jax import lax
from jax.experimental import pallas as pl
from jax.experimental.pallas import tpu as pltpu
from jax.sharding import PartitionSpec as P

TOP_K = 2
EPS = 1e-06
MESH = pl.DeviceIdType.MESH
BF = jnp.bfloat16
F32 = jnp.float32
HIGH = lax.Precision.HIGHEST
NS = jax.named_scope


def mm(a, b, dims=((1,), (0,)), precision=None):
    return lax.dot_general(
        a, b, (dims, ((), ())), preferred_element_type=F32, precision=precision
    )


def kernel(
    cfg,
    q_hbm,
    fi_hbm,
    v_hbm,
    og_hbm,
    ds_hbm,
    ff_hbm,
    hg_hbm,
    x_hbm,
    mg_hbm,
    rt_hbm,
    rw_hbm,
    wm_hbm,
    wg_hbm,
    wu_hbm,
    wd_hbm,
    mixed_hbm,
    moe_hbm,
    q_ref,
    fi_ref,
    v_ref,
    og_ref,
    ds_ref,
    ff_ref,
    hg_ref,
    x_ref,
    mg_ref,
    rt_ref,
    rw_ref,
    mixed_ref,
    moe_ref,
    wm,
    wg,
    wu,
    wd,
    dispn,
    dispf,
    xs,
    hid,
    snd_p,
    rs_p,
    own,
    snd_y,
    rs_y,
    fin,
    ret,
    wpn,
    wpf,
    kx_s,
    kx_r,
    kc_s,
    kc_r,
    pair,
    carry,
    intra,
    qdec,
    ho,
    in_sem,
    out_sem,
    w_sem,
    sends,
    n_rs,
    a_rs,
    gn_rs,
    gy_rs,
    gp_rs,
    rp_rs,
    ry_rs,
    b_rs,
    kx_rs,
    kc_rs,
    hy_rs,
    hp_rs,
):
    ep, tp, cap, near = cfg
    far = ep - near
    ny = tp // 2
    me = lax.axis_index("ep")
    t = lax.axis_index("tp")
    y = t // 2
    c = t % 2
    mate = y * 2 + (1 - c)
    rows, dim = x_ref.shape
    width = dim // tp
    slots = ep * cap
    hidden_units = wg.shape[1]
    heads = ds_ref.shape[0]
    hs = hg_ref.shape[1]
    hw = q_ref.shape[1]
    hpn = ho.shape[2]
    cw = hw // hpn
    bits = ep.bit_length() - 1
    me_bits = [lax.rem(lax.div(me, 2**k), 2) for k in range(bits)]
    zi = lax.div(me, 2)
    nz = ep // 2
    xb = me_bits[0]

    def ring(a, n):
        return lax.rem(a + n, n)

    def up_y(dy):
        return ring(y + dy, ny)

    def dn_y(dy):
        return ring(y - dy, ny)

    def peer(mask):
        out = 0
        for k in range(bits):
            out = out + (1 - me_bits[k] if (mask >> k) & 1 else me_bits[k]) * 2**k
        return out

    def peer_dyn(mask):
        out = 0
        for k in range(bits):
            m = lax.rem(lax.div(mask, 2**k), 2)
            out = out + lax.rem(me_bits[k] + m, 2) * 2**k
        return out

    def rc(src, dst, ss, rs, e, j):
        return pltpu.make_async_remote_copy(
            src_ref=src, dst_ref=dst, send_sem=ss, recv_sem=rs, device_id=(e, j), device_id_type=MESH
        )

    loads = [
        pltpu.make_async_copy(wg_hbm.at[0], wg, w_sem.at[0]),
        pltpu.make_async_copy(wu_hbm.at[0], wu, w_sem.at[1]),
        pltpu.make_async_copy(wd_hbm.at[0], wd, w_sem.at[2]),
        pltpu.make_async_copy(wm_hbm, wm, w_sem.at[3]),
    ]
    small = {}
    pairs = (
        ("rt", rt_hbm, rt_ref),
        ("x", x_hbm, x_ref),
        ("mg", mg_hbm, mg_ref),
        ("fi", fi_hbm, fi_ref),
        ("ff", ff_hbm, ff_ref),
        ("ds", ds_hbm, ds_ref),
        ("v", v_hbm, v_ref),
        ("q", q_hbm, q_ref),
        ("rw", rw_hbm, rw_ref),
        ("og", og_hbm, og_ref),
        ("hg", hg_hbm, hg_ref),
    )
    for i, (name, src, dst) in enumerate(pairs):
        small[name] = pltpu.make_async_copy(src, dst, in_sem.at[i])
    for name in ("rt", "x", "mg"):
        small[name].start()
    barrier = pltpu.get_barrier_semaphore()
    for d in range(1, ep):
        pl.semaphore_signal(barrier, inc=1, device_id=(ring(me + d, ep), t), device_id_type=MESH)
    for dy in range(1, ny):
        pl.semaphore_signal(barrier, inc=1, device_id=(me, up_y(dy) * 2 + c), device_id_type=MESH)
    pl.semaphore_signal(barrier, inc=1, device_id=(me, mate), device_id_type=MESH)

    gn, gf = near // 2, far // 2
    inner = lax.rem(me_bits[1] + me_bits[2], 2) if bits > 2 else 0
    early = [near + gf * (1 - inner) + i for i in range(gf)]
    late = [near + gf * inner + i for i in range(gf)]
    hf = gf // 2
    groups = [
        [(p, True) for p in range(gn)],
        [(p, False) for p in early],
        [(p, False) for p in late[:hf]] + [(p, True) for p in range(gn, near)],
        [(p, False) for p in late[hf:]],
    ]
    first_of = [sum(len(g) for g in groups[:i]) for i in range(len(groups))]

    kinds = ("near", "far", "gn", "gy", "gp", "rp", "ry", "back", "kx", "kc", "hy", "hp")
    sem = {kind: sends.at[i] for i, kind in enumerate(kinds)}

    def near_a2a(p, yy):
        return rc(dispn.at[yy, p], xs.at[yy, c, p], sem["near"], n_rs.at[p, yy], peer(p), t)

    def near_a2a_in(p, yy):
        r = xs.at[yy, c, p]
        return rc(r, r, sem["near"], n_rs.at[p, yy], me, mate)

    def far_a2a(p):
        return rc(dispf.at[p - near], xs.at[y, c, p], sem["far"], a_rs.at[p - near], peer_dyn(p), t)

    def far_a2a_in(p):
        r = xs.at[y, c, p]
        return rc(r, r, sem["far"], a_rs.at[p - near], me, mate)

    def near_p(p, yy):
        r = xs.at[yy, c, p]
        return rc(r, r, sem["gn"], gn_rs.at[p, yy], me, mate)

    def near_p_in(p, yy):
        r = xs.at[yy, 1 - c, p]
        return rc(r, r, sem["gn"], gn_rs.at[p, yy], me, mate)

    def gat_y(p, dy):
        r = xs.at[y, c, p]
        return rc(r, r, sem["gy"], gy_rs.at[dy - 1, p - near], me, up_y(dy) * 2 + c)

    def gat_y_in(p, dy):
        r = xs.at[dn_y(dy), c, p]
        return rc(r, r, sem["gy"], gy_rs.at[dy - 1, p - near], me, mate)

    def gat_p(p, dy):
        r = xs.at[dn_y(dy), c, p]
        return rc(r, r, sem["gp"], gp_rs.at[dy, p - near], me, mate)

    def gat_p_in(p, dy):
        r = xs.at[dn_y(dy), 1 - c, p]
        return rc(r, r, sem["gp"], gp_rs.at[dy, p - near], me, mate)

    def take_near(p):
        with NS(f"take_near{p}"):
            for yy in range(ny):
                if p:
                    near_a2a_in(p, yy).wait_recv()
                near_p(p, yy).start()

    def far_of(g):
        return [p for p, is_near in groups[g] if not is_near]

    def take_far(g, lo=0, hi=ep):
        for p in far_of(g)[lo:hi]:
            with NS(f"take_far{g}"):
                far_a2a_in(p).wait_recv()
                for dy in range(1, ny):
                    gat_y(p, dy).start()
                gat_p(p, 0).start()

    def relay_far(g, lo=0, hi=ep):
        for p in far_of(g)[lo:hi]:
            with NS(f"relay_far{g}"):
                for dy in range(1, ny):
                    gat_y_in(p, dy).wait_recv()
                    gat_p(p, dy).start()

    def arrived(g):
        with NS(f"arrived{g}"):
            for p, is_near in groups[g]:
                if is_near:
                    for yy in range(ny):
                        near_p_in(p, yy).wait_recv()
                else:
                    for dy in range(ny):
                        gat_p_in(p, dy).wait_recv()

    with NS("rt_wait"):
        small["rt"].wait()
    with NS("route"):
        i_r = lax.broadcasted_iota(jnp.int32, (rows, rows), 0)
        i_c = lax.broadcasted_iota(jnp.int32, (rows, rows), 1)
        hr = max(8, ep)
        p_row = lax.broadcasted_iota(jnp.int32, (hr, rows), 0)
        pos, hot = [], []
        for k in range(TOP_K):
            r = jnp.bitwise_xor(rt_ref[k : k + 1, :], me)
            pos.append(r)
            hot.append((p_row == r).astype(F32))
        before = mm(sum(hot).astype(BF), (i_r < i_c).astype(F32).astype(BF))
        slot = []
        for k in range(TOP_K):
            rank = jnp.sum(before * hot[k], axis=0, keepdims=True).astype(jnp.int32)
            slot.append(pos[k] * cap + rank)
        s_row = lax.broadcasted_iota(jnp.int32, (slots, rows), 0)
        hits = [s_row == slot[k] for k in range(TOP_K)]
        pick = jnp.where(hits[0], 1.0, jnp.where(hits[1], 1.0, 0.0)).astype(BF)
    with NS("x_wait"):
        small["x"].wait()
        small["mg"].wait()
        for name in ("fi", "ff", "ds", "v", "q", "rw", "og", "hg"):
            small[name].start()
    with NS("norm"):
        xf = x_ref[...].astype(F32)
        inv = lax.rsqrt(jnp.mean(xf * xf, axis=1, keepdims=True) + EPS)

        def normed(yy):
            cols = pl.ds(pl.multiple_of((yy * 2 + c) * width, width), width)
            return (x_ref[:, cols].astype(F32) * inv * mg_ref[:, cols]).astype(BF)

    nr = near * cap
    with NS("disp_near"):
        for yy in range(ny):
            out = mm(pick[0:nr], normed(yy)).astype(BF).reshape(near, cap, width)
            dispn[yy] = out
            xs[yy, c, 0] = out[0]
    with NS("bar"):
        pl.semaphore_wait(barrier, ep - 1 + ny)
    def near_send(p):
        for yy in range(ny):
            near_a2a(p, yy).start()

    for p in range(1, gn):
        near_send(p)
    with NS("disp_far"):
        dispf[...] = mm(pick[nr:], normed(y)).astype(BF).reshape(far, cap, width)
    for i in range(gf):
        for p in (early[i], late[i]):
            far_a2a(p).start()
    for p in range(gn, near - 1):
        near_send(p)
    take_near(0)

    causal = i_r >= i_c
    tri = causal.astype(F32)

    def mix_all_decay():
        fl = ff_ref[...]
        fx = fi_ref[...].astype(F32)
        forget = fl + (1.0 - fl) * jax.nn.sigmoid(fx)
        return mm(tri, jnp.log(forget), precision=HIGH)

    def state_x(h):
        return rc(kx_s.at[h], kx_r.at[h], sem["kx"], kx_rs.at[h], peer(1), t)

    def mix_head(h, run, s_col, s_row):
        hc = slice(h * hs, (h + 1) * hs)
        lr = run[:, hc]
        sc = s_col[:, h : h + 1]
        sr = s_row[h : h + 1, :]
        key = (1.0 - ff_ref[:, hc]) * jax.nn.sigmoid(-fi_ref[:, hc].astype(F32))
        v = v_ref[:, hc]
        l_end = lr[rows - 1 : rows, :]
        s_end = sc[rows - 1 : rows, :]
        kd = (key * jnp.exp(l_end - lr + (s_end - sc))).astype(BF)
        kx_s[h, 0:hs, :] = mm(v, kd, ((0,), (0,))).astype(BF)
        kx_s[h, hs : hs + 16, :] = jnp.broadcast_to(jnp.exp(l_end + s_end), (16, hs)).astype(BF)
        state_x(h).start()
        q = q_ref[:, hc].astype(F32) * jnp.exp(lr)
        scores = mm(q.astype(BF), (key * jnp.exp(-lr)).astype(BF), ((1,), (1,)))
        scores = jnp.where(causal, scores * jnp.exp(jnp.minimum(sc - sr, 0.0)), 0.0)
        intra[:, hc] = mm(scores.astype(BF), v)
        qdec[:, hc] = (q * jnp.exp(sc)).astype(BF)

    with NS("mix_wait"):
        for name in ("fi", "ff", "ds", "v", "q", "rw", "og", "hg"):
            small[name].wait()
        for load in loads:
            load.start()
    with NS("decay"):
        run = mix_all_decay()
        s_col = mm(tri, ds_ref[...], ((1,), (1,)), HIGH)
        s_rows = mm(ds_ref[...], tri, ((1,), (1,)), HIGH)
    for h in range(heads):
        with NS(f"head{h}"):
            mix_head(h, run, s_col, s_rows)
    with NS("weights"):
        wp = jnp.where(hits[0], rw_ref[0:1, :], jnp.where(hits[1], rw_ref[1:2, :], 0.0))
        wpn[...] = wp[0:nr].T.astype(BF)
        wpf[...] = wp[nr:].T.astype(BF)

    def chain_copy(h):
        return rc(kc_s.at[h], kc_r.at[h], sem["kc"], kc_rs.at[h], ring(me + 2, ep), t)

    def pair_states():
        for h in range(heads):
            state_x(h).wait_recv()
            mine = kx_s[h].astype(F32)
            other = kx_r[h].astype(F32)
            one = jnp.where(xb == 0, mine, other)
            two = jnp.where(xb == 0, other, mine)
            a_two = two[hs : hs + 1]
            both = a_two * one[0:hs] + two[0:hs]
            pair[h, 0:hs, :] = both
            pair[h, hs : hs + 8, :] = a_two * one[hs : hs + 8]

            @pl.when(zi == 0)
            def _():
                carry[h] = jnp.where(xb == 0, 0.0, other[0:hs]).astype(BF)
                kc_s[h] = both.astype(BF)
                chain_copy(h).start()

    def chain(s):
        @pl.when(zi == s)
        def _():
            for h in range(heads):
                chain_copy(h).wait_recv()
                p = kc_r[h].astype(F32)
                if s + 1 < nz:
                    kc_s[h] = (pair[h, hs : hs + 1, :] * p + pair[h, 0:hs, :]).astype(BF)
                    chain_copy(h).start()
                other = kx_r[h].astype(F32)
                carry[h] = jnp.where(xb == 0, p, other[hs : hs + 1] * p + other[0:hs]).astype(BF)

    def ho_y(p, dy):
        r = ho.at[y, c, p]
        return rc(r, r, sem["hy"], hy_rs.at[p, dy - 1], me, up_y(dy) * 2 + c)

    def ho_y_in(p, dy):
        r = ho.at[dn_y(dy), c, p]
        return rc(r, r, sem["hy"], hy_rs.at[p, dy - 1], me, mate)

    def ho_p(p, dy):
        r = ho.at[dn_y(dy), c, p]
        return rc(r, r, sem["hp"], hp_rs.at[p, dy], me, mate)

    def ho_p_in(p, dy):
        r = ho.at[dn_y(dy), 1 - c, p]
        return rc(r, r, sem["hp"], hp_rs.at[p, dy], me, mate)

    def mix_close(lo=0, hi=ep):
        for p in range(hpn)[lo:hi]:
            with NS("close"):
                for i in range(cw // hs):
                    h = p * (cw // hs) + i
                    hc = slice(h * hs, (h + 1) * hs)
                    o = intra[:, hc] + mm(qdec[:, hc], carry[h], ((1,), (1,)))
                    iv = lax.rsqrt(jnp.mean(o * o, axis=1, keepdims=True) + EPS)
                    g = og_ref[:, hc].astype(F32)
                    ho[y, c, p, :, i * hs : (i + 1) * hs] = (
                        o * iv * hg_ref[...] * (g * jax.nn.sigmoid(g))
                    ).astype(BF)
                for dy in range(1, ny):
                    ho_y(p, dy).start()
                ho_p(p, 0).start()

    def ho_relay():
        with NS("ho_relay"):
            for p in range(hpn):
                for dy in range(1, ny):
                    ho_y_in(p, dy).wait_recv()
                    ho_p(p, dy).start()

    def project():
        with NS("ho_wait"):
            for p in range(hpn):
                for dy in range(ny):
                    ho_p_in(p, dy).wait_recv()
        with NS("proj"):
            acc = jnp.zeros(mixed_ref.shape, F32)
            for j in range(tp):
                for p in range(hpn):
                    k0 = j * hw + p * cw
                    acc += mm(ho[j // 2, j % 2, p], wm[k0 : k0 + cw, :])
            mixed_ref[...] = acc.astype(BF)
            pltpu.make_async_copy(mixed_ref, mixed_hbm, out_sem.at[0]).start()

    ft = min(256, hidden_units)

    tiles = hidden_units // ft

    def first(g, between=None):
        if between is None:
            first_part(g, 0, tiles)
        else:
            first_part(g, 0, tiles // 2)
            between()
            first_part(g, tiles // 2, tiles)

    def first_part(g, lo, hi):
        with NS(f"first{g}"):
            gr = len(groups[g]) * cap

            def tile(k, _):
                fc = pl.ds(pl.multiple_of(k * ft, ft), ft)
                gate = jnp.zeros((gr, ft), F32)
                up = jnp.zeros((gr, ft), F32)
                for j in range(tp):
                    a = jnp.concatenate([xs[j // 2, j % 2, p] for p, _ in groups[g]], axis=0)
                    gate += mm(a, wg[j * width : (j + 1) * width, fc])
                    up += mm(a, wu[j * width : (j + 1) * width, fc])
                hid[0:gr, fc] = (gate * jax.nn.sigmoid(gate) * up).astype(BF)
                return 0

            lax.fori_loop(lo, hi, tile, 0)

    def red_p(g, dy):
        rs = pl.ds(first_of[g] * cap, len(groups[g]) * cap)
        return rc(snd_p.at[dy, rs], rs_p.at[dy, rs], sem["rp"], rp_rs.at[g, dy], me, mate)

    def red_y(b, dy):
        rs = pl.ds(b * cap, cap)
        return rc(
            snd_y.at[dy, rs], rs_y.at[dy, rs], sem["ry"], ry_rs.at[b, dy - 1], me, up_y(dy) * 2 + c
        )

    order = list(range(1, ny)) + [0]

    def second(g):
        r0 = first_of[g] * cap
        gr = len(groups[g]) * cap

        def down(dy, core):
            col = up_y(dy) * 2 + core
            return mm(hid[0:gr], wd[:, pl.ds(pl.multiple_of(col * width, width), width)])

        with NS(f"second{g}"):
            for dy in order:
                snd_p[dy, r0 : r0 + gr] = down(dy, 1 - c).astype(BF)
                red_p(g, dy).start()
            for dy in order:
                own[dy, r0 : r0 + gr] = down(dy, c)

    def reduce_wait(g):
        with NS(f"reduce_wait{g}"):
            for dy in range(1, ny):
                red_p(g, dy).wait_recv()

    def reduce_y(g, i):
        b = first_of[g] + i
        rr = slice(b * cap, (b + 1) * cap)
        with NS(f"reduce_y{g}"):
            for dy in range(1, ny):
                snd_y[dy, rr] = (own[dy, rr] + rs_p[dy, rr].astype(F32)).astype(BF)
                red_y(b, dy).start()

    def reduce_all(g):
        reduce_wait(g)
        for i in range(len(groups[g])):
            reduce_y(g, i)

    def back(g, i):
        p, is_near = groups[g][i]
        b = first_of[g] + i
        dest = peer(p) if is_near else peer_dyn(p)
        return rc(fin.at[b], ret.at[p], sem["back"], b_rs.at[p], dest, t)

    def give_wait(g):
        with NS(f"give_wait{g}"):
            red_p(g, 0).wait_recv()

    def give_back(g, i):
        b = first_of[g] + i
        rr = slice(b * cap, (b + 1) * cap)
        with NS(f"give_back{g}"):
            total = own[0, rr] + rs_p[0, rr].astype(F32)
            for dy in range(1, ny):
                red_y(b, dy).wait_recv()
                total += rs_y[dy, rr].astype(F32)
            if b == 0:
                ret[0] = total.astype(BF)
            else:
                fin[b] = total.astype(BF)
                back(g, i).start()

    def give_all(g):
        give_wait(g)
        for i in range(len(groups[g])):
            give_back(g, i)

    def back_in(p):
        return rc(fin.at[p], ret.at[p], sem["back"], b_rs.at[p], me, mate)

    def chain_at(lo, hi):
        with NS(f"chain{lo}"):
            for s in range(lo, min(hi, nz)):
                chain(s)

    nl = len(far_of(2))
    for p in range(1, gn):
        take_near(p)
    take_far(1, 0, hf)
    with NS("loads"):
        for load in loads[:3]:
            load.wait()
    arrived(0)
    first(0)
    take_far(1, hf)
    second(0)
    reduce_wait(0)
    reduce_y(0, 0)
    relay_far(1, 0, hf)
    with NS("pair_states"):
        pair_states()
    near_send(near - 1)
    relay_far(1, hf)
    for i in range(1, gn):
        reduce_y(0, i)
    take_far(2)
    arrived(1)
    first(1, lambda: chain_at(1, 2))
    for p in range(gn, near):
        take_near(p)
    take_far(3)
    second(1)
    relay_far(2)
    reduce_all(1)
    chain_at(2, 3)
    give_all(0)
    arrived(2)
    first(2, lambda: relay_far(3))
    chain_at(3, nz)
    mix_close(0, 1)
    give_wait(1)
    for i in range(hf):
        give_back(1, i)
    second(2)
    reduce_wait(2)
    for i in range(nl + 1):
        reduce_y(2, i)
    for i in range(hf, gf):
        give_back(1, i)
    arrived(3)
    first(3)
    second(3)
    reduce_all(3)
    for i in range(nl + 1, len(groups[2])):
        reduce_y(2, i)
    mix_close(1)
    give_wait(2)
    for i in range(nl + 1):
        give_back(2, i)
    give_all(3)
    for i in range(nl + 1, len(groups[2])):
        give_back(2, i)
    ho_relay()
    loads[3].wait()
    project()
    with NS("near_back"):
        for p in range(1, near):
            back_in(p).wait_recv()
    with NS("comb_near"):
        res = mm(wpn[...], ret[0:near].reshape(nr, width))
    with NS("far_back"):
        for p in range(near, ep):
            back_in(p).wait_recv()
    with NS("comb_far"):
        res += mm(wpf[...], ret[near:].reshape(slots - nr, width))
        moe_ref[...] = res.astype(BF)
        pltpu.make_async_copy(moe_ref, moe_hbm, out_sem.at[1]).start()

    with NS("drain"):
        sent = {
            "near": dispn.at[:, 1:near],
            "far": dispf,
            "gn": dispn,
            "gy": snd_y.at[1:ny, 0 : far * cap],
            "gp": snd_y.at[:, 0 : far * cap],
            "rp": snd_p,
            "ry": snd_y.at[1:ny],
            "back": fin.at[1:ep],
            "kx": kx_s,
            "hy": ho.at[1:ny, 0],
            "hp": ho.at[:, 0],
        }
        for kind, r in sent.items():
            rc(r, r, sem[kind], b_rs.at[0], me, mate).wait_send()
        pl.when(zi + 1 < nz)(lambda: rc(kc_s, kc_s, sem["kc"], b_rs.at[0], me, mate).wait_send())
        pltpu.make_async_copy(mixed_ref, mixed_hbm, out_sem.at[0]).wait()
        pltpu.make_async_copy(moe_ref, moe_hbm, out_sem.at[1]).wait()


def emit(a_ref, b_ref, a_out, b_out, held, sem):
    copies = [
        (
            pltpu.make_async_copy(src, held.at[i], sem.at[i, 0]),
            pltpu.make_async_copy(held.at[i], dst, sem.at[i, 1]),
        )
        for i, (src, dst) in enumerate(((a_ref, a_out), (b_ref, b_out)))
    ]
    for take, _ in copies:
        take.start()
    for take, give in copies:
        take.wait()
        give.start()
    for _, give in copies:
        give.wait()


def body(ep, tp, *args):
    (q, fi, v, og, ds, ff, hg, wm, x, mg, rt, rw, wg, wu, wd) = args
    rows, dim = x.shape
    capacity = 5 * rows * TOP_K // (4 * ep)
    cap = -(-capacity // 16) * 16
    near = min(4, ep // 2)
    ny = tp // 2
    width = dim // tp
    heads = ds.shape[1]
    hs = hg.shape[0]
    hw = q.shape[1]
    hpn = max(1, heads // 2)
    fu = wg.shape[2]
    slots = ep * cap
    gmax = max(near // 2, (ep - near) // 2) * cap + near // 2 * cap
    vm = pltpu.VMEM
    dma = pltpu.SemaphoreType.DMA
    operands = (q, fi, v, og, ds.T, ff[None, :], hg[None, :], x, mg[None, :], rt.T, rw.T)
    scratch = [vm(a.shape, a.dtype) for a in operands] + [
        vm((rows, width), BF),
        vm((rows, width), BF),
        vm(wm.shape, BF),
        vm(wg.shape[1:], BF),
        vm(wu.shape[1:], BF),
        vm(wd.shape[1:], BF),
        vm((ny, near, cap, width), BF),
        vm((ep - near, cap, width), BF),
        vm((ny, 2, ep, cap, width), BF),
        vm((gmax, fu), BF),
        vm((ny, slots, width), BF),
        vm((ny, slots, width), BF),
        vm((ny, slots, width), F32),
        vm((ny, slots, width), BF),
        vm((ny, slots, width), BF),
        vm((ep, cap, width), BF),
        vm((ep, cap, width), BF),
        vm((rows, near * cap), BF),
        vm((rows, slots - near * cap), BF),
        vm((heads, hs + 16, hs), BF),
        vm((heads, hs + 16, hs), BF),
        vm((heads, hs, hs), BF),
        vm((heads, hs, hs), BF),
        vm((heads, hs + 8, hs), F32),
        vm((heads, hs, hs), BF),
        vm((rows, hw), F32),
        vm((rows, hw), BF),
        vm((ny, 2, hpn, rows, hw // hpn), BF),
        dma((len(operands),)),
        dma((2,)),
        dma((4,)),
        dma((12,)),
        dma((near, ny)),
        dma((ep - near,)),
        dma((near, ny)),
        dma((ny - 1, ep - near)),
        dma((ny, ep - near)),
        dma((4, ny)),
        dma((ep, ny - 1)),
        dma((ep,)),
        dma((heads,)),
        dma((heads,)),
        dma((hpn, ny - 1)),
        dma((hpn, ny)),
    ]
    out = jax.ShapeDtypeStruct((rows, width), BF)
    in_any = pl.BlockSpec(memory_space=pl.ANY)
    made = pl.pallas_call(
        functools.partial(kernel, (ep, tp, cap, near)),
        out_shape=(out, out),
        in_specs=[in_any] * 15,
        out_specs=(in_any, in_any),
        scratch_shapes=scratch,
        compiler_params=pltpu.CompilerParams(
            collective_id=0, has_side_effects=True, vmem_limit_bytes=60 * 1024 * 1024
        ),
    )(*operands, wm, wg, wu, wd)
    return pl.pallas_call(
        emit,
        out_shape=(out, out),
        in_specs=[in_any] * 2,
        out_specs=(in_any, in_any),
        scratch_shapes=[vm((2, rows, width), BF), dma((2, 2))],
        name="emit",
    )(*made)


def solution(mesh):
    placed = (
        P("ep", "tp"),
        P("ep", "tp"),
        P("ep", "tp"),
        P("ep", "tp"),
        P("ep", "tp"),
        P("tp"),
        P(),
        P(None, "tp"),
        P("ep", None),
        P(),
        P("ep", None),
        P("ep", None),
        P("ep", None, "tp"),
        P("ep", None, "tp"),
        P("ep", "tp", None),
    )
    return jax.shard_map(
        functools.partial(body, mesh.shape["ep"], mesh.shape["tp"]),
        mesh=mesh,
        in_specs=placed,
        out_specs=(P("ep", "tp"), P("ep", "tp")),
        check_vma=False,
    )
```

```python
import functools

import jax
import jax.numpy as jnp
from jax import lax
from jax.experimental import pallas as pl
from jax.experimental.pallas import tpu as pltpu
from jax.sharding import PartitionSpec as P

TOP_K = 2
EPS = 1e-06
MESH = pl.DeviceIdType.MESH
BF = jnp.bfloat16
F32 = jnp.float32
HIGH = lax.Precision.HIGHEST
NS = jax.named_scope


def mm(a, b, dims=((1,), (0,)), precision=None):
    return lax.dot_general(
        a, b, (dims, ((), ())), preferred_element_type=F32, precision=precision
    )


def kernel(
    cfg,
    q_hbm,
    fi_hbm,
    v_hbm,
    og_hbm,
    ds_hbm,
    ff_hbm,
    hg_hbm,
    x_hbm,
    mg_hbm,
    rt_hbm,
    rw_hbm,
    wm_hbm,
    wg_hbm,
    wu_hbm,
    wd_hbm,
    mixed_hbm,
    moe_hbm,
    q_ref,
    fi_ref,
    v_ref,
    og_ref,
    ds_ref,
    ff_ref,
    hg_ref,
    x_ref,
    mg_ref,
    rt_ref,
    rw_ref,
    mixed_ref,
    moe_ref,
    wm,
    wg,
    wu,
    wd,
    dispn,
    dispf,
    xs,
    hid,
    snd_p,
    rs_p,
    own,
    snd_y,
    rs_y,
    fin,
    ret,
    wpn,
    wpf,
    kx_s,
    kx_r,
    kc_s,
    kc_r,
    pair,
    carry,
    intra,
    qdec,
    ho,
    proj,
    moe_part,
    in_sem,
    out_sem,
    w_sem,
    sends,
    n_rs,
    a_rs,
    gn_rs,
    gy_rs,
    gp_rs,
    rp_rs,
    ry_rs,
    b_rs,
    kx_rs,
    kc_rs,
    hy_rs,
    hp_rs,
):
    ep, tp, cap, near = cfg
    far = ep - near
    ny = tp // 2
    me = lax.axis_index("ep")
    t = lax.axis_index("tp")
    y = t // 2
    c = t % 2
    mate = y * 2 + (1 - c)
    rows, dim = x_ref.shape
    width = dim // tp
    slots = ep * cap
    hidden_units = wg.shape[1]
    heads = ds_ref.shape[0]
    hs = hg_ref.shape[1]
    hw = q_ref.shape[1]
    hpn = ho.shape[2]
    cw = hw // hpn
    bits = ep.bit_length() - 1
    me_bits = [lax.rem(lax.div(me, 2**k), 2) for k in range(bits)]
    zi = lax.div(me, 2)
    nz = ep // 2
    xb = me_bits[0]

    def ring(a, n):
        return lax.rem(a + n, n)

    def up_y(dy):
        return ring(y + dy, ny)

    def dn_y(dy):
        return ring(y - dy, ny)

    def peer(mask):
        out = 0
        for k in range(bits):
            out = out + (1 - me_bits[k] if (mask >> k) & 1 else me_bits[k]) * 2**k
        return out

    def peer_dyn(mask):
        out = 0
        for k in range(bits):
            m = lax.rem(lax.div(mask, 2**k), 2)
            out = out + lax.rem(me_bits[k] + m, 2) * 2**k
        return out

    def rc(src, dst, ss, rs, e, j):
        return pltpu.make_async_remote_copy(
            src_ref=src, dst_ref=dst, send_sem=ss, recv_sem=rs, device_id=(e, j), device_id_type=MESH
        )

    loads = [
        pltpu.make_async_copy(wg_hbm.at[0], wg, w_sem.at[0]),
        pltpu.make_async_copy(wu_hbm.at[0], wu, w_sem.at[1]),
        pltpu.make_async_copy(wd_hbm.at[0], wd, w_sem.at[2]),
        pltpu.make_async_copy(wm_hbm, wm, w_sem.at[3]),
    ]
    small = {}
    pairs = (
        ("rt", rt_hbm, rt_ref),
        ("x", x_hbm, x_ref),
        ("mg", mg_hbm, mg_ref),
        ("fi", fi_hbm, fi_ref),
        ("ff", ff_hbm, ff_ref),
        ("ds", ds_hbm, ds_ref),
        ("v", v_hbm, v_ref),
        ("q", q_hbm, q_ref),
        ("rw", rw_hbm, rw_ref),
        ("og", og_hbm, og_ref),
        ("hg", hg_hbm, hg_ref),
    )
    for i, (name, src, dst) in enumerate(pairs):
        small[name] = pltpu.make_async_copy(src, dst, in_sem.at[i])
    for name in ("rt", "x", "mg"):
        small[name].start()
    barrier = pltpu.get_barrier_semaphore()
    for d in range(1, ep):
        pl.semaphore_signal(barrier, inc=1, device_id=(ring(me + d, ep), t), device_id_type=MESH)
    for dy in range(1, ny):
        pl.semaphore_signal(barrier, inc=1, device_id=(me, up_y(dy) * 2 + c), device_id_type=MESH)
    pl.semaphore_signal(barrier, inc=1, device_id=(me, mate), device_id_type=MESH)

    gn, gf = near // 2, far // 2
    inner = lax.rem(me_bits[1] + me_bits[2], 2) if bits > 2 else 0
    early = [near + gf * (1 - inner) + i for i in range(gf)]
    late = [near + gf * inner + i for i in range(gf)]
    hf = gf // 2
    groups = [
        [(p, True) for p in range(gn)],
        [(p, False) for p in early[:hf]],
        [(p, False) for p in early[hf:]],
        [(p, False) for p in late[:hf]] + [(p, True) for p in range(gn, gn + gn // 2)],
        [(p, False) for p in late[hf:]] + [(p, True) for p in range(gn + gn // 2, near)],
    ]
    first_of = [sum(len(g) for g in groups[:i]) for i in range(len(groups))]

    kinds = ("near", "far", "gn", "gy", "gp", "rp", "ry", "back", "kx", "kc", "hy", "hp")
    sem = {kind: sends.at[i] for i, kind in enumerate(kinds)}

    def near_a2a(p, yy):
        return rc(dispn.at[yy, p], xs.at[yy, c, p], sem["near"], n_rs.at[p, yy], peer(p), t)

    def near_a2a_in(p, yy):
        r = xs.at[yy, c, p]
        return rc(r, r, sem["near"], n_rs.at[p, yy], me, mate)

    def far_a2a(p):
        return rc(dispf.at[p - near], xs.at[y, c, p], sem["far"], a_rs.at[p - near], peer_dyn(p), t)

    def far_a2a_in(p):
        r = xs.at[y, c, p]
        return rc(r, r, sem["far"], a_rs.at[p - near], me, mate)

    def near_p(p, yy):
        r = xs.at[yy, c, p]
        return rc(r, r, sem["gn"], gn_rs.at[p, yy], me, mate)

    def near_p_in(p, yy):
        r = xs.at[yy, 1 - c, p]
        return rc(r, r, sem["gn"], gn_rs.at[p, yy], me, mate)

    def gat_y(p, dy):
        r = xs.at[y, c, p]
        return rc(r, r, sem["gy"], gy_rs.at[dy - 1, p - near], me, up_y(dy) * 2 + c)

    def gat_y_in(p, dy):
        r = xs.at[dn_y(dy), c, p]
        return rc(r, r, sem["gy"], gy_rs.at[dy - 1, p - near], me, mate)

    def gat_p(p, dy):
        r = xs.at[dn_y(dy), c, p]
        return rc(r, r, sem["gp"], gp_rs.at[dy, p - near], me, mate)

    def gat_p_in(p, dy):
        r = xs.at[dn_y(dy), 1 - c, p]
        return rc(r, r, sem["gp"], gp_rs.at[dy, p - near], me, mate)

    def take_near(p):
        with NS(f"take_near{p}"):
            for yy in range(ny):
                if p:
                    near_a2a_in(p, yy).wait_recv()
                near_p(p, yy).start()

    def far_of(g):
        return [p for p, is_near in groups[g] if not is_near]

    def take_far(g, lo=0, hi=ep):
        for p in far_of(g)[lo:hi]:
            with NS(f"take_far{g}"):
                far_a2a_in(p).wait_recv()
                for dy in range(1, ny):
                    gat_y(p, dy).start()
                gat_p(p, 0).start()

    def relay_far(g, lo=0, hi=ep):
        for p in far_of(g)[lo:hi]:
            with NS(f"relay_far{g}"):
                for dy in range(1, ny):
                    gat_y_in(p, dy).wait_recv()
                    gat_p(p, dy).start()

    def arrived(g):
        with NS(f"arrived{g}"):
            for p, is_near in groups[g]:
                if is_near:
                    for yy in range(ny):
                        near_p_in(p, yy).wait_recv()
                else:
                    for dy in range(ny):
                        gat_p_in(p, dy).wait_recv()

    with NS("rt_wait"):
        small["rt"].wait()
    with NS("route"):
        i_r = lax.broadcasted_iota(jnp.int32, (rows, rows), 0)
        i_c = lax.broadcasted_iota(jnp.int32, (rows, rows), 1)
        hr = max(8, ep)
        p_row = lax.broadcasted_iota(jnp.int32, (hr, rows), 0)
        pos, hot = [], []
        for k in range(TOP_K):
            r = jnp.bitwise_xor(rt_ref[k : k + 1, :], me)
            pos.append(r)
            hot.append((p_row == r).astype(F32))
        before = mm(sum(hot).astype(BF), (i_r < i_c).astype(F32).astype(BF))
        slot = []
        for k in range(TOP_K):
            rank = jnp.sum(before * hot[k], axis=0, keepdims=True).astype(jnp.int32)
            slot.append(pos[k] * cap + rank)
        s_row = lax.broadcasted_iota(jnp.int32, (slots, rows), 0)
        hits = [s_row == slot[k] for k in range(TOP_K)]
        pick = jnp.where(hits[0], 1.0, jnp.where(hits[1], 1.0, 0.0)).astype(BF)
    with NS("x_wait"):
        small["x"].wait()
        small["mg"].wait()
        for name in ("fi", "ff", "ds", "v", "q", "rw", "og", "hg"):
            small[name].start()
    with NS("norm"):
        xf = x_ref[...].astype(F32)
        inv = lax.rsqrt(jnp.mean(xf * xf, axis=1, keepdims=True) + EPS)

        def normed(yy):
            cols = pl.ds(pl.multiple_of((yy * 2 + c) * width, width), width)
            return (x_ref[:, cols].astype(F32) * inv * mg_ref[:, cols]).astype(BF)

    nr = near * cap

    def near_rows(lo, hi):
        for yy in range(ny):
            out = mm(pick[lo * cap : hi * cap], rows_of[yy]).astype(BF).reshape(hi - lo, cap, width)
            dispn[yy, lo:hi] = out
            if lo == 0:
                xs[yy, c, 0] = out[0]

    def near_send(p):
        for yy in range(ny):
            near_a2a(p, yy).start()

    with NS("disp_near"):
        rows_of = [normed(yy) for yy in range(ny)]
        near_rows(0, gn)
    with NS("bar"):
        pl.semaphore_wait(barrier, ep - 1 + ny)
    for p in range(1, gn):
        near_send(p)
    with NS("disp_far"):
        dispf[...] = mm(pick[nr:], normed(y)).astype(BF).reshape(far, cap, width)
    for i in range(gf):
        for p in (early[i], late[i]):
            far_a2a(p).start()
    with NS("disp_near"):
        near_rows(gn, near)
    take_near(0)

    causal = i_r >= i_c
    tri = causal.astype(F32)

    def mix_all_decay():
        fl = ff_ref[...]
        fx = fi_ref[...].astype(F32)
        forget = fl + (1.0 - fl) * jax.nn.sigmoid(fx)
        return mm(tri, jnp.log(forget), precision=HIGH)

    def state_x(h):
        return rc(kx_s.at[h], kx_r.at[h], sem["kx"], kx_rs.at[h], peer(1), t)

    def mix_head(h, run, s_col, s_row):
        hc = slice(h * hs, (h + 1) * hs)
        lr = run[:, hc]
        sc = s_col[:, h : h + 1]
        sr = s_row[h : h + 1, :]
        key = (1.0 - ff_ref[:, hc]) * jax.nn.sigmoid(-fi_ref[:, hc].astype(F32))
        v = v_ref[:, hc]
        l_end = lr[rows - 1 : rows, :]
        s_end = sc[rows - 1 : rows, :]
        kd = (key * jnp.exp(l_end - lr + (s_end - sc))).astype(BF)
        kx_s[h, 0:hs, :] = mm(v, kd, ((0,), (0,))).astype(BF)
        kx_s[h, hs : hs + 16, :] = jnp.broadcast_to(jnp.exp(l_end + s_end), (16, hs)).astype(BF)
        state_x(h).start()
        q = q_ref[:, hc].astype(F32) * jnp.exp(lr)
        scores = mm(q.astype(BF), (key * jnp.exp(-lr)).astype(BF), ((1,), (1,)))
        scores = jnp.where(causal, scores * jnp.exp(jnp.minimum(sc - sr, 0.0)), 0.0)
        intra[:, hc] = mm(scores.astype(BF), v)
        qdec[:, hc] = (q * jnp.exp(sc)).astype(BF)

    with NS("mix_wait"):
        for name in ("fi", "ff", "ds", "v", "q", "rw", "og", "hg"):
            small[name].wait()
        for load in loads:
            load.start()
    with NS("decay"):
        run = mix_all_decay()
        s_col = mm(tri, ds_ref[...], ((1,), (1,)), HIGH)
        s_rows = mm(ds_ref[...], tri, ((1,), (1,)), HIGH)
    for h in range(heads):
        with NS(f"head{h}"):
            mix_head(h, run, s_col, s_rows)
    with NS("weights"):
        wp = jnp.where(hits[0], rw_ref[0:1, :], jnp.where(hits[1], rw_ref[1:2, :], 0.0))
        wpn[...] = wp[0:nr].T.astype(BF)
        wpf[...] = wp[nr:].T.astype(BF)

    def chain_copy(h):
        return rc(kc_s.at[h], kc_r.at[h], sem["kc"], kc_rs.at[h], ring(me + 2, ep), t)

    def pair_states():
        for h in range(heads):
            state_x(h).wait_recv()
            mine = kx_s[h].astype(F32)
            other = kx_r[h].astype(F32)
            one = jnp.where(xb == 0, mine, other)
            two = jnp.where(xb == 0, other, mine)
            a_two = two[hs : hs + 1]
            both = a_two * one[0:hs] + two[0:hs]
            pair[h, 0:hs, :] = both
            pair[h, hs : hs + 8, :] = a_two * one[hs : hs + 8]

            @pl.when(zi == 0)
            def _():
                carry[h] = jnp.where(xb == 0, 0.0, other[0:hs]).astype(BF)
                kc_s[h] = both.astype(BF)
                chain_copy(h).start()

    def chain(s):
        @pl.when(zi == s)
        def _():
            for h in range(heads):
                chain_copy(h).wait_recv()
                p = kc_r[h].astype(F32)
                if s + 1 < nz:
                    kc_s[h] = (pair[h, hs : hs + 1, :] * p + pair[h, 0:hs, :]).astype(BF)
                    chain_copy(h).start()
                other = kx_r[h].astype(F32)
                carry[h] = jnp.where(xb == 0, p, other[hs : hs + 1] * p + other[0:hs]).astype(BF)

    def ho_y(p, dy):
        r = ho.at[y, c, p]
        return rc(r, r, sem["hy"], hy_rs.at[p, dy - 1], me, up_y(dy) * 2 + c)

    def ho_y_in(p, dy):
        r = ho.at[dn_y(dy), c, p]
        return rc(r, r, sem["hy"], hy_rs.at[p, dy - 1], me, mate)

    def ho_p(p, dy):
        r = ho.at[dn_y(dy), c, p]
        return rc(r, r, sem["hp"], hp_rs.at[p, dy], me, mate)

    def ho_p_in(p, dy):
        r = ho.at[dn_y(dy), 1 - c, p]
        return rc(r, r, sem["hp"], hp_rs.at[p, dy], me, mate)

    def mix_close(lo=0, hi=ep):
        for p in range(hpn)[lo:hi]:
            with NS("close"):
                for i in range(cw // hs):
                    h = p * (cw // hs) + i
                    hc = slice(h * hs, (h + 1) * hs)
                    o = intra[:, hc] + mm(qdec[:, hc], carry[h], ((1,), (1,)))
                    iv = lax.rsqrt(jnp.mean(o * o, axis=1, keepdims=True) + EPS)
                    g = og_ref[:, hc].astype(F32)
                    ho[y, c, p, :, i * hs : (i + 1) * hs] = (
                        o * iv * hg_ref[...] * (g * jax.nn.sigmoid(g))
                    ).astype(BF)
                for dy in range(1, ny):
                    ho_y(p, dy).start()
                ho_p(p, 0).start()

    def ho_relay(p):
        with NS("ho_relay"):
            for dy in range(1, ny):
                ho_y_in(p, dy).wait_recv()
                ho_p(p, dy).start()

    def project(lo, hi):
        with NS("ho_wait"):
            for p in range(lo, hi):
                for dy in range(ny):
                    ho_p_in(p, dy).wait_recv()
        with NS("proj"):
            acc = proj[...] if lo else jnp.zeros(proj.shape, F32)
            for j in range(tp):
                k0 = j * hw + lo * cw
                a = jnp.concatenate([ho[j // 2, j % 2, p] for p in range(lo, hi)], axis=1)
                acc += mm(a, wm[k0 : k0 + (hi - lo) * cw, :])
            if hi < hpn:
                proj[...] = acc
            else:
                mixed_ref[...] = acc.astype(BF)
                pltpu.make_async_copy(mixed_ref, mixed_hbm, out_sem.at[0]).start()

    ft = min(256, hidden_units)

    tiles = hidden_units // ft

    def first(g, between=None):
        if between is None:
            first_part(g, 0, tiles)
        else:
            first_part(g, 0, tiles // 2)
            between()
            first_part(g, tiles // 2, tiles)

    def first_part(g, lo, hi):
        with NS(f"first{g}"):
            gr = len(groups[g]) * cap

            def tile(k, _):
                fc = pl.ds(pl.multiple_of(k * ft, ft), ft)
                gate = jnp.zeros((gr, ft), F32)
                up = jnp.zeros((gr, ft), F32)
                for j in range(tp):
                    a = jnp.concatenate([xs[j // 2, j % 2, p] for p, _ in groups[g]], axis=0)
                    gate += mm(a, wg[j * width : (j + 1) * width, fc])
                    up += mm(a, wu[j * width : (j + 1) * width, fc])
                hid[0:gr, fc] = (gate * jax.nn.sigmoid(gate) * up).astype(BF)
                return 0

            lax.fori_loop(lo, hi, tile, 0)

    def red_p(g, dy):
        rs = pl.ds(first_of[g] * cap, len(groups[g]) * cap)
        return rc(snd_p.at[dy, rs], rs_p.at[dy, rs], sem["rp"], rp_rs.at[g, dy], me, mate)

    def red_y(b, dy):
        rs = pl.ds(b * cap, cap)
        return rc(
            snd_y.at[dy, rs], rs_y.at[dy, rs], sem["ry"], ry_rs.at[b, dy - 1], me, up_y(dy) * 2 + c
        )

    order = list(range(1, ny)) + [0]

    def second(g, between=None):
        r0 = first_of[g] * cap
        gr = len(groups[g]) * cap

        def down(dy, core):
            col = up_y(dy) * 2 + core
            return mm(hid[0:gr], wd[:, pl.ds(pl.multiple_of(col * width, width), width)])

        with NS(f"second{g}"):
            for dy in order:
                snd_p[dy, r0 : r0 + gr] = down(dy, 1 - c).astype(BF)
                red_p(g, dy).start()
        if between is not None:
            between()
        with NS(f"second{g}"):
            for dy in order:
                own[dy, r0 : r0 + gr] = down(dy, c)

    def reduce_wait(g):
        with NS(f"reduce_wait{g}"):
            for dy in range(1, ny):
                red_p(g, dy).wait_recv()

    def reduce_y(g, i):
        b = first_of[g] + i
        rr = slice(b * cap, (b + 1) * cap)
        with NS(f"reduce_y{g}"):
            for dy in range(1, ny):
                snd_y[dy, rr] = (own[dy, rr] + rs_p[dy, rr].astype(F32)).astype(BF)
                red_y(b, dy).start()

    def reduce_all(g):
        reduce_wait(g)
        for i in range(len(groups[g])):
            reduce_y(g, i)

    def back(g, i):
        p, is_near = groups[g][i]
        b = first_of[g] + i
        dest = peer(p) if is_near else peer_dyn(p)
        return rc(fin.at[b], ret.at[p], sem["back"], b_rs.at[p], dest, t)

    def give_wait(g):
        with NS(f"give_wait{g}"):
            red_p(g, 0).wait_recv()

    def give_back(g, i):
        b = first_of[g] + i
        rr = slice(b * cap, (b + 1) * cap)
        with NS(f"give_back{g}"):
            total = own[0, rr] + rs_p[0, rr].astype(F32)
            for dy in range(1, ny):
                red_y(b, dy).wait_recv()
                total += rs_y[dy, rr].astype(F32)
            if b == 0:
                ret[0] = total.astype(BF)
            else:
                fin[b] = total.astype(BF)
                back(g, i).start()

    def give_all(g):
        give_wait(g)
        for i in range(len(groups[g])):
            give_back(g, i)

    def back_in(p):
        return rc(fin.at[p], ret.at[p], sem["back"], b_rs.at[p], me, mate)

    def chain_at(lo, hi):
        with NS(f"chain{lo}"):
            for s in range(lo, min(hi, nz)):
                chain(s)

    half = gn + gn // 2
    step = max(1, hpn // 2)
    for p in range(1, gn):
        take_near(p)
    take_far(1)
    with NS("loads"):
        for load in loads[:3]:
            load.wait()
    arrived(0)
    first(0)

    def between_0():
        take_far(2)
        with NS("pair_states"):
            pair_states()
        for p in range(gn, near):
            near_send(p)

    second(0, between_0)
    reduce_wait(0)
    reduce_y(0, 0)
    relay_far(1)
    for i in range(1, gn):
        reduce_y(0, i)
    take_far(3)
    arrived(1)
    first(1)
    relay_far(2)
    second(1)
    reduce_all(1)
    chain_at(1, 2)
    arrived(2)
    first(2)
    take_far(4)
    second(2)
    for p in range(gn, half):
        take_near(p)
    relay_far(3)
    reduce_all(2)
    chain_at(2, 3)
    pl.when(zi <= 2)(lambda: mix_close(0, step))
    give_all(0)
    arrived(3)

    def between_3():
        for p in range(half, near):
            take_near(p)

    first(3, between_3)
    give_all(1)
    relay_far(4)
    second(3)
    reduce_all(3)
    give_all(2)
    chain_at(3, nz)
    arrived(4)
    first(4)
    second(4)
    reduce_all(4)
    pl.when(zi > 2)(lambda: mix_close(0, step))
    mix_close(step)
    give_all(3)
    give_all(4)
    loads[3].wait()
    for lo in range(0, hpn, step):
        for p in range(lo, lo + step):
            ho_relay(p)
        project(lo, lo + step)
    with NS("near_back"):
        for p in range(1, near):
            back_in(p).wait_recv()
    with NS("comb_near"):
        moe_part[...] = mm(wpn[...], ret[0:near].reshape(nr, width))
    with NS("far_back"):
        for p in range(near, ep):
            back_in(p).wait_recv()
    with NS("comb_far"):
        res = moe_part[...] + mm(wpf[...], ret[near:].reshape(slots - nr, width))
        moe_ref[...] = res.astype(BF)
        pltpu.make_async_copy(moe_ref, moe_hbm, out_sem.at[1]).start()

    with NS("drain"):
        sent = {
            "near": dispn.at[:, 1:near],
            "far": dispf,
            "gn": dispn,
            "gy": snd_y.at[1:ny, 0 : far * cap],
            "gp": snd_y.at[:, 0 : far * cap],
            "rp": snd_p,
            "ry": snd_y.at[1:ny],
            "back": fin.at[1:ep],
            "kx": kx_s,
            "hy": ho.at[1:ny, 0],
            "hp": ho.at[:, 0],
        }
        for kind, r in sent.items():
            rc(r, r, sem[kind], b_rs.at[0], me, mate).wait_send()
        pl.when(zi + 1 < nz)(lambda: rc(kc_s, kc_s, sem["kc"], b_rs.at[0], me, mate).wait_send())
        pltpu.make_async_copy(mixed_ref, mixed_hbm, out_sem.at[0]).wait()
        pltpu.make_async_copy(moe_ref, moe_hbm, out_sem.at[1]).wait()


def emit(a_ref, b_ref, a_out, b_out, held, sem):
    copies = [
        (
            pltpu.make_async_copy(src, held.at[i], sem.at[i, 0]),
            pltpu.make_async_copy(held.at[i], dst, sem.at[i, 1]),
        )
        for i, (src, dst) in enumerate(((a_ref, a_out), (b_ref, b_out)))
    ]
    for take, _ in copies:
        take.start()
    for take, give in copies:
        take.wait()
        give.start()
    for _, give in copies:
        give.wait()


def body(ep, tp, *args):
    (q, fi, v, og, ds, ff, hg, wm, x, mg, rt, rw, wg, wu, wd) = args
    rows, dim = x.shape
    capacity = 5 * rows * TOP_K // (4 * ep)
    cap = -(-capacity // 16) * 16
    near = min(4, ep // 2)
    ny = tp // 2
    width = dim // tp
    heads = ds.shape[1]
    hs = hg.shape[0]
    hw = q.shape[1]
    hpn = heads
    fu = wg.shape[2]
    slots = ep * cap
    gmax = max(near // 2, (ep - near) // 2) * cap + near // 2 * cap
    vm = pltpu.VMEM
    dma = pltpu.SemaphoreType.DMA
    operands = (q, fi, v, og, ds.T, ff[None, :], hg[None, :], x, mg[None, :], rt.T, rw.T)
    scratch = [vm(a.shape, a.dtype) for a in operands] + [
        vm((rows, width), BF),
        vm((rows, width), BF),
        vm(wm.shape, BF),
        vm(wg.shape[1:], BF),
        vm(wu.shape[1:], BF),
        vm(wd.shape[1:], BF),
        vm((ny, near, cap, width), BF),
        vm((ep - near, cap, width), BF),
        vm((ny, 2, ep, cap, width), BF),
        vm((gmax, fu), BF),
        vm((ny, slots, width), BF),
        vm((ny, slots, width), BF),
        vm((ny, slots, width), F32),
        vm((ny, slots, width), BF),
        vm((ny, slots, width), BF),
        vm((ep, cap, width), BF),
        vm((ep, cap, width), BF),
        vm((rows, near * cap), BF),
        vm((rows, slots - near * cap), BF),
        vm((heads, hs + 16, hs), BF),
        vm((heads, hs + 16, hs), BF),
        vm((heads, hs, hs), BF),
        vm((heads, hs, hs), BF),
        vm((heads, hs + 8, hs), F32),
        vm((heads, hs, hs), BF),
        vm((rows, hw), F32),
        vm((rows, hw), BF),
        vm((ny, 2, hpn, rows, hw // hpn), BF),
        vm((rows, width), F32),
        vm((rows, width), F32),
        dma((len(operands),)),
        dma((2,)),
        dma((4,)),
        dma((12,)),
        dma((near, ny)),
        dma((ep - near,)),
        dma((near, ny)),
        dma((ny - 1, ep - near)),
        dma((ny, ep - near)),
        dma((5, ny)),
        dma((ep, ny - 1)),
        dma((ep,)),
        dma((heads,)),
        dma((heads,)),
        dma((hpn, ny - 1)),
        dma((hpn, ny)),
    ]
    out = jax.ShapeDtypeStruct((rows, width), BF)
    in_any = pl.BlockSpec(memory_space=pl.ANY)
    made = pl.pallas_call(
        functools.partial(kernel, (ep, tp, cap, near)),
        out_shape=(out, out),
        in_specs=[in_any] * 15,
        out_specs=(in_any, in_any),
        scratch_shapes=scratch,
        compiler_params=pltpu.CompilerParams(
            collective_id=0, has_side_effects=True, vmem_limit_bytes=60 * 1024 * 1024
        ),
    )(*operands, wm, wg, wu, wd)
    return pl.pallas_call(
        emit,
        out_shape=(out, out),
        in_specs=[in_any] * 2,
        out_specs=(in_any, in_any),
        scratch_shapes=[vm((2, rows, width), BF), dma((2, 2))],
        name="emit",
    )(*made)


def solution(mesh):
    placed = (
        P("ep", "tp"),
        P("ep", "tp"),
        P("ep", "tp"),
        P("ep", "tp"),
        P("ep", "tp"),
        P("tp"),
        P(),
        P(None, "tp"),
        P("ep", None),
        P(),
        P("ep", None),
        P("ep", None),
        P("ep", None, "tp"),
        P("ep", None, "tp"),
        P("ep", "tp", None),
    )
    return jax.shard_map(
        functools.partial(body, mesh.shape["ep"], mesh.shape["tp"]),
        mesh=mesh,
        in_specs=placed,
        out_specs=(P("ep", "tp"), P("ep", "tp")),
        check_vma=False,
    )
```

```python
import functools

import jax
import jax.numpy as jnp
from jax import lax
from jax.experimental import pallas as pl
from jax.experimental.pallas import tpu as pltpu
from jax.sharding import PartitionSpec as P

TOP_K = 2
EPS = 1e-06
MESH = pl.DeviceIdType.MESH
BF = jnp.bfloat16
F32 = jnp.float32
HIGH = lax.Precision.HIGHEST
NS = jax.named_scope


def mm(a, b, dims=((1,), (0,)), precision=None):
    return lax.dot_general(
        a, b, (dims, ((), ())), preferred_element_type=F32, precision=precision
    )


def kernel(
    cfg,
    q_hbm,
    fi_hbm,
    v_hbm,
    og_hbm,
    ds_hbm,
    ff_hbm,
    hg_hbm,
    x_hbm,
    mg_hbm,
    rt_hbm,
    rw_hbm,
    wm_hbm,
    wg_hbm,
    wu_hbm,
    wd_hbm,
    mixed_hbm,
    moe_hbm,
    q_ref,
    fi_ref,
    v_ref,
    og_ref,
    ds_ref,
    ff_ref,
    hg_ref,
    x_ref,
    mg_ref,
    rt_ref,
    rw_ref,
    mixed_ref,
    moe_ref,
    wm,
    wg,
    wu,
    wd,
    dispn,
    dispf,
    xs,
    hid,
    snd_p,
    rs_p,
    own,
    snd_y,
    rs_y,
    fin,
    ret,
    wpn,
    wpf,
    kx_s,
    kx_r,
    kc_s,
    kc_r,
    pair,
    carry,
    intra,
    qdec,
    ho,
    proj,
    moe_part,
    in_sem,
    out_sem,
    w_sem,
    sends,
    n_rs,
    a_rs,
    gn_rs,
    gy_rs,
    gp_rs,
    rp_rs,
    ry_rs,
    b_rs,
    kx_rs,
    kc_rs,
    hy_rs,
    hp_rs,
):
    ep, tp, cap, near = cfg
    far = ep - near
    ny = tp // 2
    me = lax.axis_index("ep")
    t = lax.axis_index("tp")
    y = t // 2
    c = t % 2
    mate = y * 2 + (1 - c)
    rows, dim = x_ref.shape
    width = dim // tp
    slots = ep * cap
    hidden_units = wg.shape[1]
    heads = ds_ref.shape[0]
    hs = hg_ref.shape[1]
    hw = q_ref.shape[1]
    hpn = ho.shape[2]
    cw = hw // hpn
    bits = ep.bit_length() - 1
    me_bits = [lax.rem(lax.div(me, 2**k), 2) for k in range(bits)]
    zi = lax.div(me, 2)
    nz = ep // 2
    xb = me_bits[0]

    def ring(a, n):
        return lax.rem(a + n, n)

    def up_y(dy):
        return ring(y + dy, ny)

    def dn_y(dy):
        return ring(y - dy, ny)

    def peer(mask):
        out = 0
        for k in range(bits):
            out = out + (1 - me_bits[k] if (mask >> k) & 1 else me_bits[k]) * 2**k
        return out

    def peer_dyn(mask):
        out = 0
        for k in range(bits):
            m = lax.rem(lax.div(mask, 2**k), 2)
            out = out + lax.rem(me_bits[k] + m, 2) * 2**k
        return out

    def rc(src, dst, ss, rs, e, j):
        return pltpu.make_async_remote_copy(
            src_ref=src, dst_ref=dst, send_sem=ss, recv_sem=rs, device_id=(e, j), device_id_type=MESH
        )

    loads = [
        pltpu.make_async_copy(wg_hbm.at[0], wg, w_sem.at[0]),
        pltpu.make_async_copy(wu_hbm.at[0], wu, w_sem.at[1]),
        pltpu.make_async_copy(wd_hbm.at[0], wd, w_sem.at[2]),
        pltpu.make_async_copy(wm_hbm, wm, w_sem.at[3]),
    ]
    small = {}
    pairs = (
        ("rt", rt_hbm, rt_ref),
        ("x", x_hbm, x_ref),
        ("mg", mg_hbm, mg_ref),
        ("fi", fi_hbm, fi_ref),
        ("ff", ff_hbm, ff_ref),
        ("ds", ds_hbm, ds_ref),
        ("v", v_hbm, v_ref),
        ("q", q_hbm, q_ref),
        ("rw", rw_hbm, rw_ref),
        ("og", og_hbm, og_ref),
        ("hg", hg_hbm, hg_ref),
    )
    for i, (name, src, dst) in enumerate(pairs):
        small[name] = pltpu.make_async_copy(src, dst, in_sem.at[i])
    for name in ("rt", "x", "mg"):
        small[name].start()
    barrier = pltpu.get_barrier_semaphore()
    for d in range(1, ep):
        pl.semaphore_signal(barrier, inc=1, device_id=(ring(me + d, ep), t), device_id_type=MESH)
    for dy in range(1, ny):
        pl.semaphore_signal(barrier, inc=1, device_id=(me, up_y(dy) * 2 + c), device_id_type=MESH)
    pl.semaphore_signal(barrier, inc=1, device_id=(me, mate), device_id_type=MESH)

    gn, gf = near // 2, far // 2
    inner = lax.rem(me_bits[1] + me_bits[2], 2) if bits > 2 else 0
    early = [near + gf * (1 - inner) + i for i in range(gf)]
    late = [near + gf * inner + i for i in range(gf)]
    hf = gf // 2
    groups = [
        [(p, True) for p in range(gn)],
        [(p, False) for p in early[:hf]],
        [(p, False) for p in early[hf:]],
        [(p, False) for p in late[:hf]] + [(p, True) for p in range(gn, gn + gn // 2)],
        [(p, False) for p in late[hf:]] + [(p, True) for p in range(gn + gn // 2, near)],
    ]
    first_of = [sum(len(g) for g in groups[:i]) for i in range(len(groups))]

    kinds = ("near", "far", "gn", "gy", "gp", "rp", "ry", "back", "kx", "kc", "hy", "hp")
    sem = {kind: sends.at[i] for i, kind in enumerate(kinds)}

    def near_a2a(p, yy):
        return rc(dispn.at[yy, p], xs.at[yy, c, p], sem["near"], n_rs.at[p, yy], peer(p), t)

    def near_a2a_in(p, yy):
        r = xs.at[yy, c, p]
        return rc(r, r, sem["near"], n_rs.at[p, yy], me, mate)

    def far_a2a(p):
        return rc(dispf.at[p - near], xs.at[y, c, p], sem["far"], a_rs.at[p - near], peer_dyn(p), t)

    def far_a2a_in(p):
        r = xs.at[y, c, p]
        return rc(r, r, sem["far"], a_rs.at[p - near], me, mate)

    def near_p(p, yy):
        r = xs.at[yy, c, p]
        return rc(r, r, sem["gn"], gn_rs.at[p, yy], me, mate)

    def near_p_in(p, yy):
        r = xs.at[yy, 1 - c, p]
        return rc(r, r, sem["gn"], gn_rs.at[p, yy], me, mate)

    def gat_y(p, dy):
        r = xs.at[y, c, p]
        return rc(r, r, sem["gy"], gy_rs.at[dy - 1, p - near], me, up_y(dy) * 2 + c)

    def gat_y_in(p, dy):
        r = xs.at[dn_y(dy), c, p]
        return rc(r, r, sem["gy"], gy_rs.at[dy - 1, p - near], me, mate)

    def gat_p(p, dy):
        r = xs.at[dn_y(dy), c, p]
        return rc(r, r, sem["gp"], gp_rs.at[dy, p - near], me, mate)

    def gat_p_in(p, dy):
        r = xs.at[dn_y(dy), 1 - c, p]
        return rc(r, r, sem["gp"], gp_rs.at[dy, p - near], me, mate)

    def take_near(p):
        with NS(f"take_near{p}"):
            for yy in range(ny):
                if p:
                    near_a2a_in(p, yy).wait_recv()
                near_p(p, yy).start()

    def far_of(g):
        return [p for p, is_near in groups[g] if not is_near]

    def take_far(g, lo=0, hi=ep):
        for p in far_of(g)[lo:hi]:
            with NS(f"take_far{g}"):
                far_a2a_in(p).wait_recv()
                for dy in range(1, ny):
                    gat_y(p, dy).start()
                gat_p(p, 0).start()

    def relay_far(g, lo=0, hi=ep):
        for p in far_of(g)[lo:hi]:
            with NS(f"relay_far{g}"):
                for dy in range(1, ny):
                    gat_y_in(p, dy).wait_recv()
                    gat_p(p, dy).start()

    def arrived(g):
        with NS(f"arrived{g}"):
            for p, is_near in groups[g]:
                if is_near:
                    for yy in range(ny):
                        near_p_in(p, yy).wait_recv()
                else:
                    for dy in range(ny):
                        gat_p_in(p, dy).wait_recv()

    with NS("rt_wait"):
        small["rt"].wait()
    with NS("route"):
        i_r = lax.broadcasted_iota(jnp.int32, (rows, rows), 0)
        i_c = lax.broadcasted_iota(jnp.int32, (rows, rows), 1)
        hr = max(8, ep)
        p_row = lax.broadcasted_iota(jnp.int32, (hr, rows), 0)
        pos, hot = [], []
        for k in range(TOP_K):
            r = jnp.bitwise_xor(rt_ref[k : k + 1, :], me)
            pos.append(r)
            hot.append((p_row == r).astype(F32))
        before = mm(sum(hot).astype(BF), (i_r < i_c).astype(F32).astype(BF))
        slot = []
        for k in range(TOP_K):
            rank = jnp.sum(before * hot[k], axis=0, keepdims=True).astype(jnp.int32)
            slot.append(pos[k] * cap + rank)
        s_row = lax.broadcasted_iota(jnp.int32, (slots, rows), 0)
        hits = [s_row == slot[k] for k in range(TOP_K)]
        pick = jnp.where(hits[0], 1.0, jnp.where(hits[1], 1.0, 0.0)).astype(BF)
    with NS("x_wait"):
        small["x"].wait()
        small["mg"].wait()
        for name in ("fi", "ff", "ds", "v", "q", "rw", "og", "hg"):
            small[name].start()
    with NS("norm"):
        xf = x_ref[...].astype(F32)
        inv = lax.rsqrt(jnp.mean(xf * xf, axis=1, keepdims=True) + EPS)

        def normed(yy):
            cols = pl.ds(pl.multiple_of((yy * 2 + c) * width, width), width)
            return (x_ref[:, cols].astype(F32) * inv * mg_ref[:, cols]).astype(BF)

    nr = near * cap

    def near_rows(lo, hi):
        for yy in range(ny):
            out = mm(pick[lo * cap : hi * cap], rows_of[yy]).astype(BF).reshape(hi - lo, cap, width)
            dispn[yy, lo:hi] = out
            if lo == 0:
                xs[yy, c, 0] = out[0]

    def near_send(p):
        for yy in range(ny):
            near_a2a(p, yy).start()

    with NS("disp_near"):
        rows_of = [normed(yy) for yy in range(ny)]
        near_rows(0, gn)
    with NS("bar"):
        pl.semaphore_wait(barrier, ep - 1 + ny)
    for p in range(1, gn):
        near_send(p)
    with NS("disp_far"):
        dispf[...] = mm(pick[nr:], normed(y)).astype(BF).reshape(far, cap, width)
    for i in range(gf):
        for p in (early[i], late[i]):
            far_a2a(p).start()
    with NS("disp_near"):
        near_rows(gn, near)
    take_near(0)

    causal = i_r >= i_c
    tri = causal.astype(F32)

    def mix_all_decay():
        fl = ff_ref[...]
        fx = fi_ref[...].astype(F32)
        forget = fl + (1.0 - fl) * jax.nn.sigmoid(fx)
        return mm(tri, jnp.log(forget), precision=HIGH)

    def state_x(h):
        return rc(kx_s.at[h], kx_r.at[h], sem["kx"], kx_rs.at[h], peer(1), t)

    def mix_head(h, run, s_col, s_row):
        hc = slice(h * hs, (h + 1) * hs)
        lr = run[:, hc]
        sc = s_col[:, h : h + 1]
        sr = s_row[h : h + 1, :]
        key = (1.0 - ff_ref[:, hc]) * jax.nn.sigmoid(-fi_ref[:, hc].astype(F32))
        v = v_ref[:, hc]
        l_end = lr[rows - 1 : rows, :]
        s_end = sc[rows - 1 : rows, :]
        kd = (key * jnp.exp(l_end - lr + (s_end - sc))).astype(BF)
        kx_s[h, 0:hs, :] = mm(v, kd, ((0,), (0,))).astype(BF)
        kx_s[h, hs : hs + 16, :] = jnp.broadcast_to(jnp.exp(l_end + s_end), (16, hs)).astype(BF)
        state_x(h).start()
        q = q_ref[:, hc].astype(F32) * jnp.exp(lr)
        scores = mm(q.astype(BF), (key * jnp.exp(-lr)).astype(BF), ((1,), (1,)))
        scores = jnp.where(causal, scores * jnp.exp(jnp.minimum(sc - sr, 0.0)), 0.0)
        intra[:, hc] = mm(scores.astype(BF), v)
        qdec[:, hc] = (q * jnp.exp(sc)).astype(BF)

    with NS("mix_wait"):
        for name in ("fi", "ff", "ds", "v", "q", "rw", "og", "hg"):
            small[name].wait()
        for load in loads:
            load.start()
    with NS("decay"):
        run = mix_all_decay()
        s_col = mm(tri, ds_ref[...], ((1,), (1,)), HIGH)
        s_rows = mm(ds_ref[...], tri, ((1,), (1,)), HIGH)
    for h in range(heads):
        with NS(f"head{h}"):
            mix_head(h, run, s_col, s_rows)
    with NS("weights"):
        wp = jnp.where(hits[0], rw_ref[0:1, :], jnp.where(hits[1], rw_ref[1:2, :], 0.0))
        wpn[...] = wp[0:nr].T.astype(BF)
        wpf[...] = wp[nr:].T.astype(BF)

    def chain_copy(h):
        return rc(kc_s.at[h], kc_r.at[h], sem["kc"], kc_rs.at[h], ring(me + 2, ep), t)

    def pair_states():
        for h in range(heads):
            state_x(h).wait_recv()
            mine = kx_s[h].astype(F32)
            other = kx_r[h].astype(F32)
            one = jnp.where(xb == 0, mine, other)
            two = jnp.where(xb == 0, other, mine)
            a_two = two[hs : hs + 1]
            both = a_two * one[0:hs] + two[0:hs]
            pair[h, 0:hs, :] = both
            pair[h, hs : hs + 8, :] = a_two * one[hs : hs + 8]

            @pl.when(zi == 0)
            def _():
                carry[h] = jnp.where(xb == 0, 0.0, other[0:hs]).astype(BF)
                kc_s[h] = both.astype(BF)
                chain_copy(h).start()

    def chain(s):
        @pl.when(zi == s)
        def _():
            for h in range(heads):
                chain_copy(h).wait_recv()
                p = kc_r[h].astype(F32)
                if s + 1 < nz:
                    kc_s[h] = (pair[h, hs : hs + 1, :] * p + pair[h, 0:hs, :]).astype(BF)
                    chain_copy(h).start()
                other = kx_r[h].astype(F32)
                carry[h] = jnp.where(xb == 0, p, other[hs : hs + 1] * p + other[0:hs]).astype(BF)

    def ho_y(p, dy):
        r = ho.at[y, c, p]
        return rc(r, r, sem["hy"], hy_rs.at[p, dy - 1], me, up_y(dy) * 2 + c)

    def ho_y_in(p, dy):
        r = ho.at[dn_y(dy), c, p]
        return rc(r, r, sem["hy"], hy_rs.at[p, dy - 1], me, mate)

    def ho_p(p, dy):
        r = ho.at[dn_y(dy), c, p]
        return rc(r, r, sem["hp"], hp_rs.at[p, dy], me, mate)

    def ho_p_in(p, dy):
        r = ho.at[dn_y(dy), 1 - c, p]
        return rc(r, r, sem["hp"], hp_rs.at[p, dy], me, mate)

    def mix_close(lo=0, hi=ep):
        for p in range(hpn)[lo:hi]:
            with NS("close"):
                for i in range(cw // hs):
                    h = p * (cw // hs) + i
                    hc = slice(h * hs, (h + 1) * hs)
                    o = intra[:, hc] + mm(qdec[:, hc], carry[h], ((1,), (1,)))
                    iv = lax.rsqrt(jnp.mean(o * o, axis=1, keepdims=True) + EPS)
                    g = og_ref[:, hc].astype(F32)
                    ho[y, c, p, :, i * hs : (i + 1) * hs] = (
                        o * iv * hg_ref[...] * (g * jax.nn.sigmoid(g))
                    ).astype(BF)
                for dy in range(1, ny):
                    ho_y(p, dy).start()
                ho_p(p, 0).start()

    def ho_relay(p):
        with NS("ho_relay"):
            for dy in range(1, ny):
                ho_y_in(p, dy).wait_recv()
                ho_p(p, dy).start()

    def project(lo, hi):
        with NS("ho_wait"):
            for p in range(lo, hi):
                for dy in range(ny):
                    ho_p_in(p, dy).wait_recv()
        with NS("proj"):
            acc = proj[...] if lo else jnp.zeros(proj.shape, F32)
            for j in range(tp):
                k0 = j * hw + lo * cw
                a = jnp.concatenate([ho[j // 2, j % 2, p] for p in range(lo, hi)], axis=1)
                acc += mm(a, wm[k0 : k0 + (hi - lo) * cw, :])
            if hi < hpn:
                proj[...] = acc
            else:
                mixed_ref[...] = acc.astype(BF)
                pltpu.make_async_copy(mixed_ref, mixed_hbm, out_sem.at[0]).start()

    ft = min(256, hidden_units)

    tiles = hidden_units // ft

    def first(g, between=None):
        if between is None:
            first_part(g, 0, tiles)
        else:
            first_part(g, 0, tiles // 2)
            between()
            first_part(g, tiles // 2, tiles)

    def first_part(g, lo, hi):
        with NS(f"first{g}"):
            gr = len(groups[g]) * cap

            def tile(k, _):
                fc = pl.ds(pl.multiple_of(k * ft, ft), ft)
                gate = jnp.zeros((gr, ft), F32)
                up = jnp.zeros((gr, ft), F32)
                for j in range(tp):
                    a = jnp.concatenate([xs[j // 2, j % 2, p] for p, _ in groups[g]], axis=0)
                    gate += mm(a, wg[j * width : (j + 1) * width, fc])
                    up += mm(a, wu[j * width : (j + 1) * width, fc])
                hid[0:gr, fc] = (gate * jax.nn.sigmoid(gate) * up).astype(BF)
                return 0

            lax.fori_loop(lo, hi, tile, 0)

    def red_p(g, dy):
        rs = pl.ds(first_of[g] * cap, len(groups[g]) * cap)
        return rc(snd_p.at[dy, rs], rs_p.at[dy, rs], sem["rp"], rp_rs.at[g, dy], me, mate)

    def red_y(b, dy):
        rs = pl.ds(b * cap, cap)
        return rc(
            snd_y.at[dy, rs], rs_y.at[dy, rs], sem["ry"], ry_rs.at[b, dy - 1], me, up_y(dy) * 2 + c
        )

    order = list(range(1, ny)) + [0]

    def second(g, between=None):
        r0 = first_of[g] * cap
        gr = len(groups[g]) * cap

        def down(dy, core):
            col = up_y(dy) * 2 + core
            return mm(hid[0:gr], wd[:, pl.ds(pl.multiple_of(col * width, width), width)])

        with NS(f"second{g}"):
            for dy in order:
                snd_p[dy, r0 : r0 + gr] = down(dy, 1 - c).astype(BF)
                red_p(g, dy).start()
        if between is not None:
            between()
        with NS(f"second{g}"):
            for dy in order:
                own[dy, r0 : r0 + gr] = down(dy, c)

    def reduce_wait(g):
        with NS(f"reduce_wait{g}"):
            for dy in range(1, ny):
                red_p(g, dy).wait_recv()

    def reduce_y(g, i):
        b = first_of[g] + i
        rr = slice(b * cap, (b + 1) * cap)
        with NS(f"reduce_y{g}"):
            for dy in range(1, ny):
                snd_y[dy, rr] = (own[dy, rr] + rs_p[dy, rr].astype(F32)).astype(BF)
                red_y(b, dy).start()

    def reduce_all(g):
        reduce_wait(g)
        for i in range(len(groups[g])):
            reduce_y(g, i)

    def back(g, i):
        p, is_near = groups[g][i]
        b = first_of[g] + i
        dest = peer(p) if is_near else peer_dyn(p)
        return rc(fin.at[b], ret.at[p], sem["back"], b_rs.at[p], dest, t)

    def give_wait(g):
        with NS(f"give_wait{g}"):
            red_p(g, 0).wait_recv()

    def give_back(g, i):
        b = first_of[g] + i
        rr = slice(b * cap, (b + 1) * cap)
        with NS(f"give_back{g}"):
            total = own[0, rr] + rs_p[0, rr].astype(F32)
            for dy in range(1, ny):
                red_y(b, dy).wait_recv()
                total += rs_y[dy, rr].astype(F32)
            if b == 0:
                ret[0] = total.astype(BF)
            else:
                fin[b] = total.astype(BF)
                back(g, i).start()

    def give_all(g):
        give_wait(g)
        for i in range(len(groups[g])):
            give_back(g, i)

    def back_in(p):
        return rc(fin.at[p], ret.at[p], sem["back"], b_rs.at[p], me, mate)

    def chain_at(lo, hi):
        with NS(f"chain{lo}"):
            for s in range(lo, min(hi, nz)):
                chain(s)

    half = gn + gn // 2
    step = max(1, hpn // 2)
    for p in range(1, gn):
        take_near(p)
    take_far(1)
    with NS("loads"):
        for load in loads[:3]:
            load.wait()
    arrived(0)
    first(0)

    def between_0():
        take_far(2)
        with NS("pair_states"):
            pair_states()
        for p in range(gn, near):
            near_send(p)

    second(0, between_0)
    reduce_wait(0)
    reduce_y(0, 0)
    relay_far(1)
    for i in range(1, gn):
        reduce_y(0, i)
    take_far(3)
    arrived(1)
    first(1)
    relay_far(2)
    second(1)
    reduce_all(1)
    chain_at(1, 2)
    arrived(2)
    first(2)
    take_far(4)
    second(2)
    for p in range(gn, half):
        take_near(p)
    relay_far(3)
    reduce_all(2)
    chain_at(2, 3)
    pl.when(zi <= 2)(lambda: mix_close(0, step))
    give_all(0)
    arrived(3)

    first(3)
    give_all(1)
    for p in range(half, near):
        take_near(p)
    relay_far(4)
    second(3)
    reduce_all(3)
    give_all(2)
    chain_at(3, nz)
    arrived(4)
    first(4)
    second(4)
    reduce_all(4)
    pl.when(zi > 2)(lambda: mix_close(0, step))
    mix_close(step)
    give_all(3)
    give_all(4)
    loads[3].wait()
    for lo in range(0, hpn, step):
        for p in range(lo, lo + step):
            ho_relay(p)
        project(lo, lo + step)
    with NS("near_back"):
        for p in range(1, near):
            back_in(p).wait_recv()
    with NS("comb_near"):
        moe_part[...] = mm(wpn[...], ret[0:near].reshape(nr, width))
    with NS("far_back"):
        for p in range(near, ep):
            back_in(p).wait_recv()
    with NS("comb_far"):
        far_back = ret[near:].reshape(slots - nr, width)
        for i in range(2):
            rh = slice(i * rows // 2, (i + 1) * rows // 2)
            moe_ref[rh] = (moe_part[rh] + mm(wpf[rh], far_back)).astype(BF)
            pltpu.make_async_copy(moe_ref.at[rh], moe_hbm.at[rh], out_sem.at[1 + i]).start()

    with NS("drain"):
        sent = {
            "near": dispn.at[:, 1:near],
            "far": dispf,
            "gn": dispn,
            "gy": snd_y.at[1:ny, 0 : far * cap],
            "gp": snd_y.at[:, 0 : far * cap],
            "rp": snd_p,
            "ry": snd_y.at[1:ny],
            "back": fin.at[1:ep],
            "kx": kx_s,
            "hy": ho.at[1:ny, 0],
            "hp": ho.at[:, 0],
        }
        for kind, r in sent.items():
            rc(r, r, sem[kind], b_rs.at[0], me, mate).wait_send()
        pl.when(zi + 1 < nz)(lambda: rc(kc_s, kc_s, sem["kc"], b_rs.at[0], me, mate).wait_send())
        pltpu.make_async_copy(mixed_ref, mixed_hbm, out_sem.at[0]).wait()
        for i in range(2):
            rh = slice(i * rows // 2, (i + 1) * rows // 2)
            pltpu.make_async_copy(moe_ref.at[rh], moe_hbm.at[rh], out_sem.at[1 + i]).wait()


def emit(a_ref, b_ref, a_out, b_out, held, sem):
    copies = [
        (
            pltpu.make_async_copy(src, held.at[i], sem.at[i, 0]),
            pltpu.make_async_copy(held.at[i], dst, sem.at[i, 1]),
        )
        for i, (src, dst) in enumerate(((a_ref, a_out), (b_ref, b_out)))
    ]
    for take, _ in copies:
        take.start()
    for take, give in copies:
        take.wait()
        give.start()
    for _, give in copies:
        give.wait()


def body(ep, tp, *args):
    (q, fi, v, og, ds, ff, hg, wm, x, mg, rt, rw, wg, wu, wd) = args
    rows, dim = x.shape
    capacity = 5 * rows * TOP_K // (4 * ep)
    cap = -(-capacity // 16) * 16
    near = min(4, ep // 2)
    ny = tp // 2
    width = dim // tp
    heads = ds.shape[1]
    hs = hg.shape[0]
    hw = q.shape[1]
    hpn = heads
    fu = wg.shape[2]
    slots = ep * cap
    gmax = max(near // 2, (ep - near) // 2) * cap + near // 2 * cap
    vm = pltpu.VMEM
    dma = pltpu.SemaphoreType.DMA
    operands = (q, fi, v, og, ds.T, ff[None, :], hg[None, :], x, mg[None, :], rt.T, rw.T)
    scratch = [vm(a.shape, a.dtype) for a in operands] + [
        vm((rows, width), BF),
        vm((rows, width), BF),
        vm(wm.shape, BF),
        vm(wg.shape[1:], BF),
        vm(wu.shape[1:], BF),
        vm(wd.shape[1:], BF),
        vm((ny, near, cap, width), BF),
        vm((ep - near, cap, width), BF),
        vm((ny, 2, ep, cap, width), BF),
        vm((gmax, fu), BF),
        vm((ny, slots, width), BF),
        vm((ny, slots, width), BF),
        vm((ny, slots, width), F32),
        vm((ny, slots, width), BF),
        vm((ny, slots, width), BF),
        vm((ep, cap, width), BF),
        vm((ep, cap, width), BF),
        vm((rows, near * cap), BF),
        vm((rows, slots - near * cap), BF),
        vm((heads, hs + 16, hs), BF),
        vm((heads, hs + 16, hs), BF),
        vm((heads, hs, hs), BF),
        vm((heads, hs, hs), BF),
        vm((heads, hs + 8, hs), F32),
        vm((heads, hs, hs), BF),
        vm((rows, hw), F32),
        vm((rows, hw), BF),
        vm((ny, 2, hpn, rows, hw // hpn), BF),
        vm((rows, width), F32),
        vm((rows, width), F32),
        dma((len(operands),)),
        dma((3,)),
        dma((4,)),
        dma((12,)),
        dma((near, ny)),
        dma((ep - near,)),
        dma((near, ny)),
        dma((ny - 1, ep - near)),
        dma((ny, ep - near)),
        dma((5, ny)),
        dma((ep, ny - 1)),
        dma((ep,)),
        dma((heads,)),
        dma((heads,)),
        dma((hpn, ny - 1)),
        dma((hpn, ny)),
    ]
    out = jax.ShapeDtypeStruct((rows, width), BF)
    in_any = pl.BlockSpec(memory_space=pl.ANY)
    made = pl.pallas_call(
        functools.partial(kernel, (ep, tp, cap, near)),
        out_shape=(out, out),
        in_specs=[in_any] * 15,
        out_specs=(in_any, in_any),
        scratch_shapes=scratch,
        compiler_params=pltpu.CompilerParams(
            collective_id=0, has_side_effects=True, vmem_limit_bytes=60 * 1024 * 1024
        ),
    )(*operands, wm, wg, wu, wd)
    return pl.pallas_call(
        emit,
        out_shape=(out, out),
        in_specs=[in_any] * 2,
        out_specs=(in_any, in_any),
        scratch_shapes=[vm((2, rows, width), BF), dma((2, 2))],
        name="emit",
    )(*made)


def solution(mesh):
    placed = (
        P("ep", "tp"),
        P("ep", "tp"),
        P("ep", "tp"),
        P("ep", "tp"),
        P("ep", "tp"),
        P("tp"),
        P(),
        P(None, "tp"),
        P("ep", None),
        P(),
        P("ep", None),
        P("ep", None),
        P("ep", None, "tp"),
        P("ep", None, "tp"),
        P("ep", "tp", None),
    )
    return jax.shard_map(
        functools.partial(body, mesh.shape["ep"], mesh.shape["tp"]),
        mesh=mesh,
        in_specs=placed,
        out_specs=(P("ep", "tp"), P("ep", "tp")),
        check_vma=False,
    )
```
